32 devices in a mesh: ep: 4 (over y, x), tp: 8 (over z, core).
Axes of the slice: x: 2, y: 2, z: 4, core: 2. Of those that a mesh axis runs over, the one named last changes fastest.
Arguments:
- stream: bfloat16 [64, 2048], P('ep'), may hold values from -6 to 6
- norm_gain_attn: float32 [2048], replicated, may hold values from 0.1 to 1.9
- w_query: bfloat16 [2048, 2048], P('ep', 'tp'), may hold values from -0.125 to 0.125
- w_key: bfloat16 [2048, 2048], P('ep', 'tp'), may hold values from -0.125 to 0.125
- w_value: bfloat16 [2048, 2048], P('ep', 'tp'), may hold values from -0.125 to 0.125
- w_forget: bfloat16 [2048, 16], replicated, may hold values from -0.125 to 0.125
- forget_bias: float32 [16], replicated, may hold values from -2 to 2
- key_cache: bfloat16 [64, 1024, 2048], P('ep', None, 'tp'), may hold values from -1500 to 1500
- value_cache: bfloat16 [64, 1024, 2048], P('ep', None, 'tp'), may hold values from -6 to 6
- gate_cache: float32 [64, 16, 1024], P('ep', 'tp'), may hold values from -1024 to 0, as said below
- lengths: int32 [64], P('ep'), may hold values from 128 to 1024
- w_output: bfloat16 [2048, 2048], P('tp'), may hold values from -0.125 to 0.125
- norm_gain_ffn: float32 [2048], replicated, may hold values from 0.1 to 1.9
- routes: int32 [64, 2], replicated, may hold values from 0 to 3, all different within a row; in each aligned block of 16 rows (0 to 15, 16 to 31, ...) at most 16 rows name the same one
- route_weights: float32 [64, 2], replicated, may hold values from 0.2 to 1
- w_expert_gate: bfloat16 [4, 2048, 5632], P('ep', None, 'tp'), may hold values from -0.125 to 0.125
- w_expert_up: bfloat16 [4, 2048, 5632], P('ep', None, 'tp'), may hold values from -0.125 to 0.125
- expert_down_weight: bfloat16 [4, 5632, 2048], P('ep', 'tp'), may hold values from -0.078125 to 0.078125
Outputs:
- result: bfloat16 [64, 2048], P('ep', 'tp')
The draws below stay inside these ranges and needn't reach their ends.
Inputs may be any that keep to these rules, and one draw needn't show every extreme that they name: `gate_cache`: never rises along positions. `routes`: in the rows of one index of ep no expert is named by more than 16 rows, and in some such block one is named by exactly 16.
All inputs are finite; a program needn't handle non-finite values.
Results may differ from the reference program's by a relative error of at most 0.014.
Values may be sent and summed in bfloat16 or wider, within the bound.
No kernel may reach another device: no remote copies, remote signals or barrier semaphores. Data moves between devices by JAX's collectives and lax.ppermute only.
A program may use at most 64 MiB of HBM per device.

```python
import math
import jax
import jax.numpy as jnp
import numpy as np
from jax import lax

D = 2048
HEADS = 16
HEAD_DIM = 128
FF = 5632
TOP = 2
SEQ_DEV = 16
CACHE = 1024
ATT = 2048
BATCH = 64
EXPERTS = 4
CAP = 16
N_EP = 4


def draw_key_cache(key, part):
    parts = jax.random.split(jax.random.fold_in(key, 11), 1)
    base = jax.random.normal(parts[0], (BATCH, CACHE, HEADS, HEAD_DIM), jnp.float32)
    return base.reshape(BATCH, CACHE, HEADS * HEAD_DIM).astype(jnp.bfloat16)


def draw_gate_cache(key, part):
    parts = jax.random.split(jax.random.fold_in(key, 23), 7)
    order = jax.random.permutation(parts[0], HEADS)
    fast_count = HEADS // 2
    fast = (order < fast_count)[None, :, None]
    block_factor = jnp.exp(jax.random.uniform(parts[1], (N_EP, 1, 1), jnp.float32, 0.0, math.log(4.0)))
    seq_factor = jnp.repeat(block_factor, SEQ_DEV, axis=0)
    fast_rate = jnp.exp(jax.random.uniform(parts[2], (BATCH, HEADS, 1), jnp.float32, math.log(1.0 / 50.0), math.log(1.0 / 30.0)))
    slow_rate = jnp.exp(jax.random.uniform(parts[3], (BATCH, HEADS, 1), jnp.float32, math.log(0.5), math.log(1.5))) / CACHE
    rate = jnp.where(fast, fast_rate, slow_rate) * seq_factor
    rough = jax.random.uniform(parts[4], (BATCH, HEADS, CACHE), jnp.float32, 0.0, 2.0)
    generation_iterations = -rate * rough
    sampled_locations = jax.random.randint(parts[5], (BATCH, HEADS, 3), 0, CACHE)
    stack_count = jax.random.uniform(parts[6], (BATCH, HEADS, 3), jnp.float32, math.log(0.5), math.log(0.8))
    sequence_indices = jnp.arange(CACHE)[None, None, None, :]
    clustered_sets = jnp.sum(jnp.where(sequence_indices == sampled_locations[..., None], stack_count[..., None], 0.0), axis=2)
    return jnp.cumsum(generation_iterations + clustered_sets, axis=2)


def touch_ends(drawn, rng, low, high):
    longest = drawn.shape.index(max(drawn.shape))
    spots = []
    for shift in (0, 1):
        where = [jax.random.randint(jax.random.fold_in(rng, axis), (), 0, length) for axis, length in enumerate(drawn.shape)]
        where[longest] = (where[longest] + shift) % drawn.shape[longest]
        spots.append(tuple(where))
    return drawn.at[spots[0]].set(low).at[spots[1]].set(high)


def level_of(own_key, shape, cuts, smallest, high):
    level = 1.0
    for position, blocks in cuts:
        heights = jax.random.uniform(jax.random.fold_in(jax.random.fold_in(own_key, 6), position), (blocks,), jnp.float32, smallest / len(cuts), high / len(cuts))
        level = level * jnp.repeat(jnp.exp(heights), shape[position] // blocks).reshape((-1,) + (1,) * (len(shape) - 1 - position))
    return level


def shared_out(own_key, own, number, rows, amount, top, bound, slope):
    sequence = jax.random.permutation(own_key, amount)
    packed, ordinary = shares(amount, rows * top, bound, slope, True), shares(amount, rows * top, bound, slope, False)
    places = jnp.arange(amount)

    def named(tallies, rotation):
        used = int((tallies > 0).sum())
        fixed = max(1, used // 4)
        moved = fixed + (places - fixed + rotation * (used - fixed)) % max(1, amount - fixed)
        return jnp.zeros((amount,), jnp.int32).at[sequence[jnp.where(places < fixed, places, moved)]].set(jnp.asarray(tallies, jnp.int32))

    tallies = jnp.where(number % 4 == 0, named(packed, number // 4), named(ordinary, number - number // 4 - 1))
    mixed = jax.random.permutation(jax.random.fold_in(own, 3), amount)
    donor, taker = mixed[0:amount // 2 * 2:2], mixed[1:amount // 2 * 2:2]
    margin = jnp.minimum(tallies[donor] - 1, bound - tallies[taker]) // 2
    margin = jnp.where((donor == sequence[0]) | (taker == sequence[0]) | (tallies[taker] == 0), 0, jnp.maximum(margin, 0))
    moved = jax.random.randint(jax.random.fold_in(own, 4), (amount // 2,), 0, 1 << 20) % (margin + 1)
    tallies = tallies.at[donor].add(-moved).at[taker].add(moved)
    items = jnp.searchsorted(jnp.cumsum(tallies), jnp.arange(rows * top), side="right").astype(jnp.int32)
    listing = items.reshape(top, rows).T
    listing = listing[jax.random.permutation(jax.random.fold_in(own, 1), rows)]
    rotation = jax.random.randint(jax.random.fold_in(own, 2), (rows, 1), 0, top)
    return jnp.take_along_axis(listing, (jnp.arange(top)[None, :] + rotation) % top, axis=1)


def shares(number_of, total, most, lean, full):
    portions = [(1 << 20) // math.isqrt(grade ** lean) + 1 for grade in range(1, number_of + 1)]
    largest = most if full else min(most, max(-(-total // number_of), total * portions[0] // sum(portions)))
    least = 1 if total - largest >= number_of - 1 else 0
    counts, spare = [largest] + [least] * (number_of - 1), total - largest - least * (number_of - 1)
    while spare > 0:
        movable = [i for i in range(1, number_of) if counts[i] < largest] or [i for i in range(1, number_of) if counts[i] < most]
        mass, remaining = sum([portions[i] for i in movable]), spare
        for i in movable:
            extra = min(most - counts[i], max(1, remaining * portions[i] // mass), spare)
            counts[i] = counts[i] + extra
            spare = spare - extra
    return np.array(counts)


def scatter_about(own_key, shape, spread, reach, cuts=(), held_as=jnp.bfloat16):
    result = spread * jax.random.normal(own_key, shape, jnp.float32)
    if cuts:
        result = result * level_of(own_key, shape, cuts, -0.22, 0.18)
    return jnp.clip(result, -reach, reach).astype(held_as)


def setup_inputs(seed: int = 0) -> dict:
    key_list = jax.random.split(jax.random.key(seed), 19)
    stream = scatter_about(key_list[0], (BATCH, D), 1.0, 6.0, ((0, 4),))
    norm_gain_attn = jnp.clip(1.0 + 0.18 * jax.random.normal(key_list[1], (D,), jnp.float32), 0.1, 1.9)
    w_query = scatter_about(key_list[2], (D, ATT), D ** -0.5, 0.125, ((0, 4), (1, 8)))
    w_key = scatter_about(key_list[3], (D, ATT), D ** -0.5, 0.125, ((0, 4), (1, 8)))
    w_value = scatter_about(key_list[4], (D, ATT), D ** -0.5, 0.125, ((0, 4), (1, 8)))
    w_forget = scatter_about(key_list[5], (D, HEADS), D ** -0.5, 0.125)
    forget_bias = jnp.clip(jax.random.uniform(key_list[6], (HEADS,), jnp.float32, -2.0, 2.0), -2.0, 2.0)
    key_cache = draw_key_cache(jax.random.fold_in(key_list[18], 71), 0)
    value_cache = scatter_about(key_list[8], (BATCH, CACHE, ATT), 1.0, 6.0, ((0, 4), (2, 8)))
    gate_cache = draw_gate_cache(jax.random.fold_in(key_list[18], 71), 0)
    lengths = touch_ends(jax.random.randint(key_list[10], (BATCH,), CACHE // 8, CACHE + 1), jax.random.fold_in(key_list[10], 1), CACHE // 8, CACHE).astype(jnp.int32)
    w_output = scatter_about(key_list[11], (ATT, D), ATT ** -0.5, 0.125, ((0, 8),))
    norm_gain_ffn = jnp.clip(1.0 + 0.18 * jax.random.normal(key_list[12], (D,), jnp.float32), 0.1, 1.9)
    routes_keys = jax.random.split(jax.random.fold_in(key_list[13], 1), BATCH // SEQ_DEV)
    routes_turns = jax.random.permutation(jax.random.fold_in(key_list[13], 3), BATCH // SEQ_DEV)
    routes = jax.vmap(lambda own, number: shared_out(jax.random.fold_in(key_list[13], 2), own, number, SEQ_DEV, EXPERTS, TOP, CAP, 2))(routes_keys, routes_turns).reshape((BATCH, TOP))
    route_weights = jnp.clip(jax.random.uniform(key_list[14], (BATCH, TOP), jnp.float32, 0.2, 1.0), 0.2, 1.0)
    w_expert_gate = scatter_about(key_list[15], (EXPERTS, D, FF), D ** -0.5, 0.125, ((0, 4), (2, 8)))
    w_expert_up = scatter_about(key_list[16], (EXPERTS, D, FF), D ** -0.5, 0.125, ((0, 4), (2, 8)))
    expert_down_weight = scatter_about(key_list[17], (EXPERTS, FF, D), FF ** -0.5, 0.078125, ((0, 4), (1, 8)))
    return dict(stream=stream, norm_gain_attn=norm_gain_attn, w_query=w_query, w_key=w_key, w_value=w_value, w_forget=w_forget, forget_bias=forget_bias, key_cache=key_cache, value_cache=value_cache, gate_cache=gate_cache, lengths=lengths, w_output=w_output, norm_gain_ffn=norm_gain_ffn, routes=routes, route_weights=route_weights, w_expert_gate=w_expert_gate, w_expert_up=w_expert_up, expert_down_weight=expert_down_weight)


def rms_norm(values, gain):
    floats = values.astype(jnp.float32)
    scaled = floats * lax.rsqrt(lax.optimization_barrier(jnp.mean(floats * floats, axis=-1, keepdims=True)) + 1e-06)
    return (scaled * gain).astype(jnp.bfloat16)

def attend_one(items):
    query, key_new, value_new, forget_new, keys, values, gates, length_total = items
    scale = HEAD_DIM ** (-0.5)
    query_f = query.astype(jnp.float32).reshape(HEADS, HEAD_DIM)
    keys_f = keys.astype(jnp.float32).reshape(CACHE, HEADS, HEAD_DIM)
    value_matrix_float = values.astype(jnp.float32).reshape(CACHE, HEADS, HEAD_DIM)
    sequence_indices = jnp.arange(CACHE, dtype=jnp.int32)
    is_live = sequence_indices < length_total
    last_gate = lax.optimization_barrier(jnp.sum(jnp.where(sequence_indices[None, :] == length_total - 1, gates, 0.0), axis=-1))
    scores = jnp.einsum('hd,phd->hp', query_f, keys_f) * scale + forget_new[:, None] + last_gate[:, None] - gates
    own_score = lax.optimization_barrier(jnp.sum(query_f * key_new.astype(jnp.float32).reshape(HEADS, HEAD_DIM), axis=-1)) * scale
    hidden_from_view = jnp.where(is_live[None, :], scores, -1e+30)
    largest = jnp.maximum(lax.optimization_barrier(jnp.max(hidden_from_view, axis=-1)), own_score)
    past = jnp.exp(hidden_from_view - largest[:, None])
    own_term = jnp.exp(own_score - largest)
    total = lax.optimization_barrier(jnp.sum(past, axis=-1)) + own_term
    past_weights = lax.optimization_barrier((past / total[:, None]).astype(jnp.bfloat16))
    own_weights = lax.optimization_barrier((own_term / total).astype(jnp.bfloat16))
    mixed = jnp.einsum('hp,phd->hd', past_weights.astype(jnp.float32), value_matrix_float)
    mixed = mixed + own_weights.astype(jnp.float32)[:, None] * value_new.astype(jnp.float32).reshape(HEADS, HEAD_DIM)
    return mixed.reshape(HEADS * HEAD_DIM).astype(jnp.bfloat16)

def reference(stream, norm_gain_attn, w_query, w_key, w_value, w_forget, forget_bias, key_cache, value_cache, gate_cache, lengths, w_output, norm_gain_ffn, routes, route_weights, w_expert_gate, w_expert_up, expert_down_weight):
    normed = rms_norm(stream, norm_gain_attn)
    query = jnp.dot(normed, w_query, preferred_element_type=jnp.float32).astype(jnp.bfloat16)
    key_new = jnp.dot(normed, w_key, preferred_element_type=jnp.float32).astype(jnp.bfloat16)
    value_new = jnp.dot(normed, w_value, preferred_element_type=jnp.float32).astype(jnp.bfloat16)
    forget_new = jax.nn.log_sigmoid(jnp.dot(normed, w_forget, preferred_element_type=jnp.float32) + forget_bias)
    attended = lax.map(attend_one, (query, key_new, value_new, forget_new, key_cache, value_cache, gate_cache, lengths))
    mixed = (stream.astype(jnp.float32) + jnp.dot(attended, w_output, preferred_element_type=jnp.float32)).astype(jnp.bfloat16)
    normed_ffn = rms_norm(mixed, norm_gain_ffn)
    flat_routes = routes.reshape(-1)
    flat_weights = route_weights.reshape(-1)
    owners = (jnp.arange(BATCH * TOP, dtype=jnp.int32) // TOP).astype(jnp.int32)
    slot_numbers = jnp.arange(CAP * N_EP, dtype=jnp.int32)

    def expert_step(combined, items):
        gate_w, up_w, down_w, index = items
        chosen = flat_routes == index
        chosen_count = jnp.sum(chosen.astype(jnp.int32))
        picks = jnp.nonzero(chosen, size=CAP * N_EP, fill_value=0)[0].astype(jnp.int32)
        token_ids = owners[picks]
        inputs = normed_ffn[token_ids]
        hidden = (jax.nn.silu(jnp.dot(inputs, gate_w, preferred_element_type=jnp.float32)) * jnp.dot(inputs, up_w, preferred_element_type=jnp.float32)).astype(jnp.bfloat16)
        outputs = lax.optimization_barrier(jnp.dot(hidden, down_w, preferred_element_type=jnp.float32).astype(jnp.bfloat16))
        weights = jnp.where(slot_numbers < chosen_count, flat_weights[picks], 0.0)
        return (combined.at[token_ids].add(outputs.astype(jnp.float32) * weights[:, None]), None)
    combined, _ = lax.scan(expert_step, jnp.zeros((BATCH, D), jnp.float32), (w_expert_gate, w_expert_up, expert_down_weight, jnp.arange(EXPERTS, dtype=jnp.int32)))
    return (mixed.astype(jnp.float32) + combined).astype(jnp.bfloat16)
```

```python
import jax
import jax.numpy as jnp
from jax import lax
from jax.experimental import pallas as pl
from jax.experimental.pallas import tpu as pltpu
from jax.sharding import PartitionSpec as P

F32 = jnp.float32
BF16 = jnp.bfloat16
ROWS = 8
STEP = 128
HIDDEN = -1e30


def normalized(floats, gain):
    return floats * lax.rsqrt(jnp.mean(floats * floats, axis=-1, keepdims=True) + 1e-06) * gain


def norm_kernel(stream_ref, gain_ref, out_ref):
    groups, _, width = out_ref.shape
    normed = normalized(stream_ref[...].astype(F32), gain_ref[...]).astype(BF16)
    for group in range(groups):
        out_ref[group] = normed[:, group * width : (group + 1) * width]


def project_kernel(block_ref, query_ref, key_ref, value_ref, out_ref):
    groups, count, features = block_ref.shape
    width = query_ref.shape[1]
    rows = block_ref[...].reshape(groups * count, features)
    for index, weight_ref in enumerate((query_ref, key_ref, value_ref)):
        part = jnp.dot(rows, weight_ref[...], preferred_element_type=F32)
        out_ref[:, :, index * width : (index + 1) * width] = part.reshape(groups, count, width)


def attend_kernel(
    lengths_ref,
    parts_ref,
    normed_ref,
    forget_ref,
    bias_ref,
    gates_ref,
    output_ref,
    keys_hbm,
    values_hbm,
    out_ref,
    keys_ref,
    values_ref,
    attended_ref,
    key_sems,
    value_sems,
):
    groups, count, features = normed_ref.shape
    heads = gates_ref.shape[1]
    cache_len = gates_ref.shape[2]
    width = keys_ref.shape[2]
    head_dim = width // heads
    scale = head_dim ** (-0.5)

    def copy(sequence, source, target, sems):
        live = pl.multiple_of((lengths_ref[sequence] + STEP - 1) // STEP * STEP, STEP)
        rows = pl.ds(0, live)
        return pltpu.make_async_copy(
            source.at[sequence, rows], target.at[sequence, rows], sems.at[sequence]
        )

    def key_copy(sequence):
        return copy(sequence, keys_hbm, keys_ref, key_sems)

    def value_copy(sequence):
        return copy(sequence, values_hbm, values_ref, value_sems)

    for first in range(0, count, ROWS):
        for start_copy in (key_copy, value_copy):
            for sequence in range(first, first + ROWS):
                start_copy(sequence).start()

    def clear(sequence, carry):
        length = lengths_ref[sequence]
        for start in range(STEP, cache_len, STEP):

            @pl.when(start >= length)
            def _():
                values_ref[sequence, start : start + STEP, :] = jnp.zeros((STEP, width), BF16)

        return carry

    lax.fori_loop(0, count, clear, 0)

    forget_sum = jnp.zeros((count, forget_ref.shape[1]), F32)
    for group in range(groups):
        forget_sum += jnp.dot(
            normed_ref[group],
            forget_ref[group * features : (group + 1) * features, :],
            preferred_element_type=F32,
        )
    forget_all = jax.nn.log_sigmoid(forget_sum + bias_ref[...])
    head_ids = lax.broadcasted_iota(jnp.int32, forget_all.shape, 1)
    first_head = lax.axis_index("tp") * heads
    total = parts_ref[0]
    for group in range(1, groups):
        total = total + parts_ref[group]
    query = total[:, :width].astype(BF16).astype(F32)
    key_new = total[:, width : 2 * width].astype(BF16).astype(F32)
    value_new = total[:, 2 * width :].astype(BF16).astype(F32)
    lanes = lax.broadcasted_iota(jnp.int32, (ROWS, width), 1)
    row_ids = lax.broadcasted_iota(jnp.int32, (ROWS, 1), 0)
    positions = lax.broadcasted_iota(jnp.int32, (ROWS, cache_len), 1)

    for first in range(0, count, ROWS):
        mine = slice(first, first + ROWS)
        length = jnp.zeros((ROWS, 1), jnp.int32)
        for row in range(ROWS):
            length = jnp.where(row_ids == row, lengths_ref[first + row], length)
        stacked = jnp.concatenate(
            [
                jnp.where(lanes // head_dim == head, query[mine], 0.0).astype(BF16)
                for head in range(heads)
            ],
            axis=0,
        )
        scores = [jnp.zeros((ROWS, cache_len), F32) for _ in range(heads)]
        for row in range(ROWS):
            key_copy(first + row).wait()
        for row in range(ROWS):
            products = lax.dot_general(
                stacked,
                keys_ref[first + row],
                (((1,), (1,)), ((), ())),
                preferred_element_type=F32,
            )
            for head in range(heads):
                scores[head] = jnp.where(
                    row_ids == row, products[head * ROWS : (head + 1) * ROWS], scores[head]
                )
        weights = []
        owns = []
        for head in range(heads):
            gates = gates_ref[mine, head, :]
            columns = slice(head * head_dim, (head + 1) * head_dim)
            last_gate = jnp.sum(
                jnp.where(positions == length - 1, gates, 0.0), axis=1, keepdims=True
            )
            forget_new = jnp.sum(
                jnp.where(head_ids[mine] == first_head + head, forget_all[mine], 0.0),
                axis=1,
                keepdims=True,
            )
            own_score = (
                jnp.sum(query[mine, columns] * key_new[mine, columns], axis=1, keepdims=True)
                * scale
            )
            score = scores[head] * scale + forget_new + last_gate - gates
            score = jnp.where(positions < length, score, HIDDEN)
            largest = jnp.maximum(jnp.max(score, axis=1, keepdims=True), own_score)
            past = jnp.exp(score - largest)
            own_term = jnp.exp(own_score - largest)
            norm = jnp.sum(past, axis=1, keepdims=True) + own_term
            weights.append((past / norm).astype(BF16))
            owns.append((own_term / norm).astype(BF16).astype(F32))
        weights = jnp.concatenate(weights, axis=0)
        results = [
            owns[head] * value_new[mine, head * head_dim : (head + 1) * head_dim]
            for head in range(heads)
        ]
        for row in range(ROWS):
            value_copy(first + row).wait()
        for row in range(ROWS):
            products = jnp.dot(weights, values_ref[first + row], preferred_element_type=F32)
            for head in range(heads):
                columns = slice(head * head_dim, (head + 1) * head_dim)
                results[head] = results[head] + jnp.where(
                    row_ids == row, products[head * ROWS : (head + 1) * ROWS, columns], 0.0
                )
        for head in range(heads):
            attended_ref[mine, head * head_dim : (head + 1) * head_dim] = results[head]

    attended = attended_ref[...].astype(BF16)
    pieces, _, piece = out_ref.shape
    product = jnp.dot(attended, output_ref[...], preferred_element_type=F32).astype(BF16)
    for index in range(pieces):
        out_ref[index] = product[:, index * piece : (index + 1) * piece]


def mix_kernel(parts_ref, stream_ref, mixed_ref, out_ref):
    pieces, _, piece = parts_ref.shape
    total = parts_ref[0].astype(F32)
    for index in range(1, pieces):
        total = total + parts_ref[index].astype(F32)
    mine = pl.ds(pl.multiple_of(lax.axis_index("tp") * piece, piece), piece)
    mixed = (stream_ref[:, mine].astype(F32) + total).astype(BF16)
    mixed_ref[...] = mixed
    for index in range(out_ref.shape[0]):
        out_ref[index] = mixed


def expert_kernel(
    mixed_ref, gain_ref, routes_ref, weights_ref, gate_ref, up_ref, down_ref, out_ref, rows_ref
):
    total, count, piece = mixed_ref.shape
    width = gate_ref.shape[1]
    pieces = width // piece
    groups = total // pieces
    for group in range(groups):
        blocks = [
            mixed_ref[group * pieces + index].astype(F32) for index in range(pieces)
        ]
        rows_ref[group * count : (group + 1) * count, :] = normalized(
            jnp.concatenate(blocks, axis=1), gain_ref[...]
        ).astype(BF16)
    rows = rows_ref[...]
    gated = jnp.dot(rows, gate_ref[0], preferred_element_type=F32)
    upper = jnp.dot(rows, up_ref[0], preferred_element_type=F32)
    hidden = (gated / (1.0 + jnp.exp(-gated)) * upper).astype(BF16)
    partial = jnp.dot(hidden, down_ref[0], preferred_element_type=F32)
    mine = routes_ref[...] == lax.axis_index("ep")
    share = jnp.sum(jnp.where(mine, weights_ref[...], 0.0), axis=1, keepdims=True)
    partial = (partial * share).astype(BF16)
    for group in range(groups):
        for index in range(pieces):
            out_ref[group * pieces + index] = partial[
                group * count : (group + 1) * count, index * piece : (index + 1) * piece
            ]


def finish_kernel(parts_ref, mixed_ref, out_ref):
    total = mixed_ref[...].astype(F32)
    for index in range(parts_ref.shape[0]):
        total = total + parts_ref[index].astype(F32)
    out_ref[...] = total.astype(BF16)


def shards(
    stream,
    norm_gain_attn,
    w_query,
    w_key,
    w_value,
    w_forget,
    forget_bias,
    key_cache,
    value_cache,
    gate_cache,
    lengths,
    w_output,
    norm_gain_ffn,
    routes,
    route_weights,
    w_expert_gate,
    w_expert_up,
    expert_down_weight,
):
    count, model_width = stream.shape
    groups = lax.axis_size("ep")
    pieces = lax.axis_size("tp")
    piece = model_width // pieces
    cache_len, width = key_cache.shape[1:]
    shape = jax.ShapeDtypeStruct
    in_vmem = pl.BlockSpec(memory_space=pltpu.VMEM)
    in_smem = pl.BlockSpec(memory_space=pltpu.SMEM)
    in_hbm = pl.BlockSpec(memory_space=pltpu.HBM)

    normed = pl.pallas_call(
        norm_kernel, out_shape=shape((groups, count, model_width // groups), BF16), name="norm"
    )(stream, norm_gain_attn.reshape(1, -1))
    block = lax.all_to_all(normed, "ep", 0, 0, tiled=True)
    projected = pl.pallas_call(
        project_kernel, out_shape=shape((groups, count, 3 * width), F32), name="project"
    )(block, w_query, w_key, w_value)
    parts = lax.all_to_all(projected, "ep", 0, 0, tiled=True)
    outputs = pl.pallas_call(
        attend_kernel,
        out_shape=shape((pieces, count, piece), BF16),
        in_specs=[in_smem] + [in_vmem] * 6 + [in_hbm] * 2,
        scratch_shapes=[
            pltpu.VMEM((count, cache_len, width), BF16),
            pltpu.VMEM((count, cache_len, width), BF16),
            pltpu.VMEM((count, width), F32),
            pltpu.SemaphoreType.DMA((count,)),
            pltpu.SemaphoreType.DMA((count,)),
        ],
        name="attend",
    )(
        lengths,
        parts,
        normed,
        w_forget,
        forget_bias.reshape(1, -1),
        gate_cache,
        w_output,
        key_cache,
        value_cache,
    )
    head_parts = lax.all_to_all(outputs, "tp", 0, 0, tiled=True)
    mixed, copies = pl.pallas_call(
        mix_kernel,
        out_shape=(shape((count, piece), BF16), shape((groups * pieces, count, piece), BF16)),
        name="mix",
    )(head_parts, stream)
    mixed_all = lax.all_to_all(copies, ("ep", "tp"), 0, 0, tiled=True)
    expert_parts = pl.pallas_call(
        expert_kernel,
        out_shape=shape((groups * pieces, count, piece), BF16),
        scratch_shapes=[pltpu.VMEM((groups * count, model_width), BF16)],
        name="experts",
    )(
        mixed_all,
        norm_gain_ffn.reshape(1, -1),
        routes,
        route_weights,
        w_expert_gate,
        w_expert_up,
        expert_down_weight,
    )
    returned = lax.all_to_all(expert_parts, ("ep", "tp"), 0, 0, tiled=True)
    return pl.pallas_call(finish_kernel, out_shape=shape((count, piece), BF16), name="finish")(
        returned, mixed
    )


def solution(mesh):
    placed = (
        P("ep", None),
        P(),
        P("ep", "tp"),
        P("ep", "tp"),
        P("ep", "tp"),
        P(),
        P(),
        P("ep", None, "tp"),
        P("ep", None, "tp"),
        P("ep", "tp", None),
        P("ep"),
        P("tp", None),
        P(),
        P(),
        P(),
        P("ep", None, "tp"),
        P("ep", None, "tp"),
        P("ep", "tp", None),
    )
    return jax.shard_map(
        shards, mesh=mesh, in_specs=placed, out_specs=P("ep", "tp"), check_vma=False
    )
```

```python
import jax
import jax.numpy as jnp
from jax import lax
from jax.experimental import pallas as pl
from jax.experimental.pallas import tpu as pltpu
from jax.sharding import PartitionSpec as P

F32 = jnp.float32
BF16 = jnp.bfloat16
ROWS = 8
HIDDEN = -1e30
MIB = 1 << 20
COVER = 40_000_000_000


def call(kernel, name, vmem, outs, flops=0, **options):
    return pl.pallas_call(
        kernel,
        out_shape=outs,
        name=name,
        cost_estimate=pl.CostEstimate(flops=flops, transcendentals=0, bytes_accessed=0),
        compiler_params=pltpu.CompilerParams(vmem_limit_bytes=vmem),
        **options,
    )


def dot_transposed(left, right):
    return lax.dot_general(left, right, (((1,), (1,)), ((), ())), preferred_element_type=F32)


def normalized(floats, gain):
    return floats * lax.rsqrt(jnp.mean(floats * floats, axis=-1, keepdims=True) + 1e-06) * gain


def norm_kernel(stream_ref, gain_ref, out_ref):
    groups, _, width = out_ref.shape
    normed = normalized(stream_ref[...].astype(F32), gain_ref[...]).astype(BF16)
    for group in range(groups):
        out_ref[group] = normed[:, group * width : (group + 1) * width]


def project_kernel(block_ref, query_ref, key_ref, value_ref, out_ref):
    groups, count, features = block_ref.shape
    width = query_ref.shape[1]
    rows = block_ref[...].reshape(groups * count, features)
    for index, weight_ref in enumerate((query_ref, key_ref, value_ref)):
        part = jnp.dot(rows, weight_ref[...], preferred_element_type=F32)
        out_ref[:, :, index * width : (index + 1) * width] = part.reshape(groups, count, width)


def attend_kernel(
    lengths_ref,
    parts_ref,
    normed_ref,
    forget_ref,
    bias_ref,
    gates_ref,
    output_ref,
    keys_ref,
    values_ref,
    out_ref,
    attended_ref,
):
    groups, count, features = normed_ref.shape
    heads = gates_ref.shape[1]
    cache_len = gates_ref.shape[2]
    width = keys_ref.shape[2]
    head_dim = width // heads
    scale = head_dim ** (-0.5)

    forget_sum = jnp.zeros((count, forget_ref.shape[0]), F32)
    for group in range(groups):
        forget_sum += dot_transposed(
            normed_ref[group], forget_ref[:, group * features : (group + 1) * features]
        )
    forget_all = jax.nn.log_sigmoid(forget_sum + bias_ref[...])
    head_ids = lax.broadcasted_iota(jnp.int32, forget_all.shape, 1)
    first_head = lax.axis_index("tp") * heads
    total = parts_ref[0]
    for group in range(1, groups):
        total = total + parts_ref[group]
    query = total[:, :width].astype(BF16).astype(F32)
    key_new = total[:, width : 2 * width].astype(BF16).astype(F32)
    value_new = total[:, 2 * width :].astype(BF16).astype(F32)
    lanes = lax.broadcasted_iota(jnp.int32, (ROWS, width), 1)
    row_ids = lax.broadcasted_iota(jnp.int32, (ROWS, 1), 0)
    positions = lax.broadcasted_iota(jnp.int32, (ROWS, cache_len), 1)

    for first in range(0, count, ROWS):
        mine = slice(first, first + ROWS)
        length = jnp.zeros((ROWS, 1), jnp.int32)
        for row in range(ROWS):
            length = jnp.where(row_ids == row, lengths_ref[first + row], length)
        stacked = jnp.concatenate(
            [
                jnp.where(lanes // head_dim == head, query[mine], 0.0).astype(BF16)
                for head in range(heads)
            ],
            axis=0,
        )
        scores = [jnp.zeros((ROWS, cache_len), F32) for _ in range(heads)]
        for row in range(ROWS):
            products = dot_transposed(stacked, keys_ref[first + row])
            for head in range(heads):
                scores[head] = jnp.where(
                    row_ids == row, products[head * ROWS : (head + 1) * ROWS], scores[head]
                )
        weights = []
        owns = []
        for head in range(heads):
            gates = gates_ref[mine, head, :]
            columns = slice(head * head_dim, (head + 1) * head_dim)
            last_gate = jnp.sum(
                jnp.where(positions == length - 1, gates, 0.0), axis=1, keepdims=True
            )
            forget_new = jnp.sum(
                jnp.where(head_ids[mine] == first_head + head, forget_all[mine], 0.0),
                axis=1,
                keepdims=True,
            )
            own_score = (
                jnp.sum(query[mine, columns] * key_new[mine, columns], axis=1, keepdims=True)
                * scale
            )
            score = scores[head] * scale + forget_new + last_gate - gates
            score = jnp.where(positions < length, score, HIDDEN)
            largest = jnp.maximum(jnp.max(score, axis=1, keepdims=True), own_score)
            past = jnp.exp(score - largest)
            own_term = jnp.exp(own_score - largest)
            norm = jnp.sum(past, axis=1, keepdims=True) + own_term
            weights.append((past / norm).astype(BF16))
            owns.append((own_term / norm).astype(BF16).astype(F32))
        weights = jnp.concatenate(weights, axis=0)
        results = [
            owns[head] * value_new[mine, head * head_dim : (head + 1) * head_dim]
            for head in range(heads)
        ]
        for row in range(ROWS):
            products = jnp.dot(weights, values_ref[first + row], preferred_element_type=F32)
            for head in range(heads):
                columns = slice(head * head_dim, (head + 1) * head_dim)
                results[head] = results[head] + jnp.where(
                    row_ids == row, products[head * ROWS : (head + 1) * ROWS, columns], 0.0
                )
        for head in range(heads):
            attended_ref[mine, head * head_dim : (head + 1) * head_dim] = results[head]

    attended = attended_ref[...].astype(BF16)
    pieces, _, piece = out_ref.shape
    product = jnp.dot(attended, output_ref[...], preferred_element_type=F32).astype(BF16)
    for index in range(pieces):
        out_ref[index] = product[:, index * piece : (index + 1) * piece]


def mix_kernel(parts_ref, stream_ref, mixed_ref, out_ref):
    pieces, _, piece = parts_ref.shape
    total = parts_ref[0].astype(F32)
    for index in range(1, pieces):
        total = total + parts_ref[index].astype(F32)
    mine = pl.ds(pl.multiple_of(lax.axis_index("tp") * piece, piece), piece)
    mixed = (stream_ref[:, mine].astype(F32) + total).astype(BF16)
    mixed_ref[...] = mixed
    for index in range(out_ref.shape[0]):
        out_ref[index] = mixed


def expert_kernel(
    mixed_ref, gain_ref, routes_ref, weights_ref, gate_ref, up_ref, down_ref, out_ref, rows_ref
):
    total, count, piece = mixed_ref.shape
    width = gate_ref.shape[2]
    pieces = width // piece
    groups = total // pieces
    for group in range(groups):
        blocks = [
            mixed_ref[group * pieces + index].astype(F32) for index in range(pieces)
        ]
        rows_ref[group * count : (group + 1) * count, :] = normalized(
            jnp.concatenate(blocks, axis=1), gain_ref[...]
        ).astype(BF16)
    rows = rows_ref[...]
    gated = dot_transposed(rows, gate_ref[0])
    upper = dot_transposed(rows, up_ref[0])
    hidden = (gated / (1.0 + jnp.exp(-gated)) * upper).astype(BF16)
    partial = jnp.dot(hidden, down_ref[0], preferred_element_type=F32)
    mine = routes_ref[...] == lax.axis_index("ep")
    share = jnp.sum(jnp.where(mine, weights_ref[...], 0.0), axis=0, keepdims=True)
    square = (groups * count, groups * count)
    same = lax.broadcasted_iota(jnp.int32, square, 0) == lax.broadcasted_iota(jnp.int32, square, 1)
    share = jnp.sum(jnp.where(same, share, 0.0), axis=1, keepdims=True)
    partial = (partial * share).astype(BF16)
    for group in range(groups):
        for index in range(pieces):
            out_ref[group * pieces + index] = partial[
                group * count : (group + 1) * count, index * piece : (index + 1) * piece
            ]


def finish_kernel(parts_ref, mixed_ref, out_ref):
    total = mixed_ref[...].astype(F32)
    for index in range(parts_ref.shape[0]):
        total = total + parts_ref[index].astype(F32)
    out_ref[...] = total.astype(BF16)


def shards(
    stream,
    norm_gain_attn,
    w_query,
    w_key,
    w_value,
    w_forget,
    forget_bias,
    key_cache,
    value_cache,
    gate_cache,
    lengths,
    w_output,
    norm_gain_ffn,
    routes,
    route_weights,
    w_expert_gate,
    w_expert_up,
    expert_down_weight,
):
    count, model_width = stream.shape
    groups = lax.axis_size("ep")
    pieces = lax.axis_size("tp")
    piece = model_width // pieces
    width = key_cache.shape[2]
    shape = jax.ShapeDtypeStruct
    in_vmem = pl.BlockSpec(memory_space=pltpu.VMEM)
    in_smem = pl.BlockSpec(memory_space=pltpu.SMEM)

    normed = call(
        norm_kernel,
        "norm",
        2 * MIB,
        shape((groups, count, model_width // groups), BF16),
        flops=COVER,
    )(stream, norm_gain_attn.reshape(1, -1))
    block = lax.all_to_all(normed, "ep", 0, 0, tiled=True)
    projected = call(
        project_kernel, "project", 4 * MIB, shape((groups, count, 3 * width), F32)
    )(block, w_query, w_key, w_value)
    parts = lax.all_to_all(projected, "ep", 0, 0, tiled=True)
    outputs = call(
        attend_kernel,
        "attend",
        4 * MIB,
        shape((pieces, count, piece), BF16),
        in_specs=[in_smem] + [in_vmem] * 8,
        scratch_shapes=[pltpu.VMEM((count, width), F32)],
    )(
        lengths,
        parts,
        normed,
        w_forget.T,
        forget_bias.reshape(1, -1),
        gate_cache,
        w_output,
        key_cache,
        value_cache,
    )
    head_parts = lax.all_to_all(outputs, "tp", 0, 0, tiled=True)
    mixed, copies = call(
        mix_kernel,
        "mix",
        4 * MIB,
        (shape((count, piece), BF16), shape((groups * pieces, count, piece), BF16)),
    )(head_parts, stream)
    mixed_all = lax.all_to_all(copies, ("ep", "tp"), 0, 0, tiled=True)
    expert_parts = call(
        expert_kernel,
        "experts",
        8 * MIB,
        shape((groups * pieces, count, piece), BF16),
        scratch_shapes=[pltpu.VMEM((groups * count, model_width), BF16)],
    )(
        mixed_all,
        norm_gain_ffn.reshape(1, -1),
        routes.T,
        route_weights.T,
        jnp.swapaxes(w_expert_gate, 1, 2),
        jnp.swapaxes(w_expert_up, 1, 2),
        expert_down_weight,
    )
    returned = lax.all_to_all(expert_parts, ("ep", "tp"), 0, 0, tiled=True)
    return call(finish_kernel, "finish", 4 * MIB, shape((count, piece), BF16))(returned, mixed)


def solution(mesh):
    placed = (
        P("ep", None),
        P(),
        P("ep", "tp"),
        P("ep", "tp"),
        P("ep", "tp"),
        P(),
        P(),
        P("ep", None, "tp"),
        P("ep", None, "tp"),
        P("ep", "tp", None),
        P("ep"),
        P("tp", None),
        P(),
        P(),
        P(),
        P("ep", None, "tp"),
        P("ep", None, "tp"),
        P("ep", "tp", None),
    )
    return jax.shard_map(
        shards, mesh=mesh, in_specs=placed, out_specs=P("ep", "tp"), check_vma=False
    )
```

```python
import functools

import jax
import jax.numpy as jnp
from jax import lax
from jax.experimental import pallas as pl
from jax.experimental.pallas import tpu as pltpu
from jax.sharding import PartitionSpec as P

F32 = jnp.float32
BF16 = jnp.bfloat16
ROWS = 8
HIDDEN = -1e30
MIB = 1 << 20
COVER = 40_000_000_000


def call(kernel, name, vmem, outs, flops=0, **options):
    return pl.pallas_call(
        kernel,
        out_shape=outs,
        name=name,
        cost_estimate=pl.CostEstimate(flops=flops, transcendentals=0, bytes_accessed=0),
        compiler_params=pltpu.CompilerParams(vmem_limit_bytes=vmem),
        **options,
    )


def dot_transposed(left, right):
    return lax.dot_general(left, right, (((1,), (1,)), ((), ())), preferred_element_type=F32)


def normalized(floats, gain):
    return floats * lax.rsqrt(jnp.mean(floats * floats, axis=-1, keepdims=True) + 1e-06) * gain


def exchange(items, axis, paired):
    if paired:
        size = len(items)
        return [items[0]] + [
            lax.ppermute(items[step], axis, [(one, one ^ step) for one in range(size)])
            for step in range(1, size)
        ]
    received = lax.all_to_all(jnp.stack(items), axis, 0, 0, tiled=True)
    return [received[index] for index in range(len(items))]


def norm_kernel(stream_hbm, gain_hbm, *refs, paired):
    normed_ref, *out_refs, stream_ref, gain_ref, sems = refs
    copies = [
        pltpu.make_async_copy(stream_hbm, stream_ref, sems.at[0]),
        pltpu.make_async_copy(gain_hbm, gain_ref, sems.at[1]),
    ]
    for copy in copies:
        copy.start()
    for copy in copies:
        copy.wait()
    width = out_refs[0].shape[1]
    normed_ref[...] = normalized(stream_ref[...].astype(F32), gain_ref[...]).astype(BF16)
    for index, out_ref in enumerate(out_refs):
        group = lax.axis_index("ep") ^ index if paired else index
        out_ref[...] = normed_ref[:, pl.ds(pl.multiple_of(group * width, width), width)]


def project_kernel(*refs):
    groups = (len(refs) - 3) // 2
    block_refs, weight_refs, out_refs = refs[:groups], refs[groups:-groups], refs[-groups:]
    count = block_refs[0].shape[0]
    width = weight_refs[0].shape[1]
    rows = jnp.concatenate([block_ref[...] for block_ref in block_refs], axis=0)
    for index, weight_ref in enumerate(weight_refs):
        part = jnp.dot(rows, weight_ref[...], preferred_element_type=F32)
        for group, out_ref in enumerate(out_refs):
            out_ref[:, index * width : (index + 1) * width] = part[
                group * count : (group + 1) * count
            ]


def attend_kernel(
    lengths_ref,
    normed_ref,
    forget_ref,
    bias_ref,
    gates_ref,
    output_ref,
    keys_ref,
    values_ref,
    *refs,
):
    *part_refs, out_ref, attended_ref = refs
    count = normed_ref.shape[0]
    heads = gates_ref.shape[1]
    cache_len = gates_ref.shape[2]
    width = keys_ref.shape[2]
    head_dim = width // heads
    scale = head_dim ** (-0.5)

    forget_all = jax.nn.log_sigmoid(
        dot_transposed(normed_ref[...], forget_ref[...]) + bias_ref[...]
    )
    head_ids = lax.broadcasted_iota(jnp.int32, forget_all.shape, 1)
    first_head = lax.axis_index("tp") * heads
    total = part_refs[0][...]
    for part_ref in part_refs[1:]:
        total = total + part_ref[...]
    query = total[:, :width].astype(BF16).astype(F32)
    key_new = total[:, width : 2 * width].astype(BF16).astype(F32)
    value_new = total[:, 2 * width :].astype(BF16).astype(F32)
    lanes = lax.broadcasted_iota(jnp.int32, (ROWS, width), 1)
    row_ids = lax.broadcasted_iota(jnp.int32, (ROWS, 1), 0)
    positions = lax.broadcasted_iota(jnp.int32, (ROWS, cache_len), 1)

    for first in range(0, count, ROWS):
        mine = slice(first, first + ROWS)
        length = jnp.zeros((ROWS, 1), jnp.int32)
        for row in range(ROWS):
            length = jnp.where(row_ids == row, lengths_ref[first + row], length)
        stacked = jnp.concatenate(
            [
                jnp.where(lanes // head_dim == head, query[mine], 0.0).astype(BF16)
                for head in range(heads)
            ],
            axis=0,
        )
        scores = [jnp.zeros((ROWS, cache_len), F32) for _ in range(heads)]
        for row in range(ROWS):
            products = dot_transposed(stacked, keys_ref[first + row])
            for head in range(heads):
                scores[head] = jnp.where(
                    row_ids == row, products[head * ROWS : (head + 1) * ROWS], scores[head]
                )
        weights = []
        owns = []
        for head in range(heads):
            gates = gates_ref[mine, head, :]
            columns = slice(head * head_dim, (head + 1) * head_dim)
            last_gate = jnp.sum(
                jnp.where(positions == length - 1, gates, 0.0), axis=1, keepdims=True
            )
            forget_new = jnp.sum(
                jnp.where(head_ids[mine] == first_head + head, forget_all[mine], 0.0),
                axis=1,
                keepdims=True,
            )
            own_score = (
                jnp.sum(query[mine, columns] * key_new[mine, columns], axis=1, keepdims=True)
                * scale
            )
            score = scores[head] * scale + forget_new + last_gate - gates
            score = jnp.where(positions < length, score, HIDDEN)
            largest = jnp.maximum(jnp.max(score, axis=1, keepdims=True), own_score)
            past = jnp.exp(score - largest)
            own_term = jnp.exp(own_score - largest)
            norm = jnp.sum(past, axis=1, keepdims=True) + own_term
            weights.append((past / norm).astype(BF16))
            owns.append((own_term / norm).astype(BF16).astype(F32))
        weights = jnp.concatenate(weights, axis=0)
        results = [
            owns[head] * value_new[mine, head * head_dim : (head + 1) * head_dim]
            for head in range(heads)
        ]
        for row in range(ROWS):
            products = jnp.dot(weights, values_ref[first + row], preferred_element_type=F32)
            for head in range(heads):
                columns = slice(head * head_dim, (head + 1) * head_dim)
                results[head] = results[head] + jnp.where(
                    row_ids == row, products[head * ROWS : (head + 1) * ROWS, columns], 0.0
                )
        for head in range(heads):
            attended_ref[mine, head * head_dim : (head + 1) * head_dim] = results[head]

    attended = attended_ref[...].astype(BF16)
    pieces, _, piece = out_ref.shape
    product = jnp.dot(attended, output_ref[...], preferred_element_type=F32).astype(BF16)
    for index in range(pieces):
        out_ref[index] = product[:, index * piece : (index + 1) * piece]


def mix_kernel(parts_ref, stream_ref, mixed_ref, out_ref):
    pieces, _, piece = parts_ref.shape
    half = out_ref.shape[1]
    total = parts_ref[0].astype(F32)
    for index in range(1, pieces):
        total = total + parts_ref[index].astype(F32)
    mine = pl.ds(pl.multiple_of(lax.axis_index("tp") * piece, piece), piece)
    mixed = stream_ref[:, mine].astype(F32) + total
    mixed_ref[...] = mixed.astype(BF16)
    for index in range(out_ref.shape[0]):
        core = index % 2
        out_ref[index] = mixed[core * half : (core + 1) * half].astype(BF16)


def expert_kernel(
    near_ref,
    far_ref,
    gain_ref,
    routes_ref,
    weights_ref,
    gate_ref,
    up_ref,
    down_ref,
    keep_ref,
    give_ref,
    rows_ref,
):
    total, half, piece = near_ref.shape
    width = gate_ref.shape[2]
    pieces = width // piece
    groups = total // pieces
    tokens = 2 * groups * half
    for side, side_ref in enumerate((near_ref, far_ref)):
        for group in range(groups):
            blocks = [side_ref[group * pieces + index].astype(F32) for index in range(pieces)]
            first = (side * groups + group) * half
            rows_ref[first : first + half, :] = normalized(
                jnp.concatenate(blocks, axis=1), gain_ref[...]
            )
    rows = rows_ref[...].astype(BF16)
    gated = dot_transposed(rows, gate_ref[0])
    upper = dot_transposed(rows, up_ref[0])
    hidden = (gated / (1.0 + jnp.exp(-gated)) * upper).astype(BF16)
    partial = jnp.dot(hidden, down_ref[0], preferred_element_type=F32)
    mine = routes_ref[...] == lax.axis_index("ep")
    share = jnp.sum(jnp.where(mine, weights_ref[...], 0.0), axis=0, keepdims=True)
    row = lax.broadcasted_iota(jnp.int32, (tokens, tokens), 0)
    core = (row // (groups * half)) ^ (lax.axis_index("tp") % 2)
    token = row // half % groups * (2 * half) + core * half + row % half
    same = token == lax.broadcasted_iota(jnp.int32, (tokens, tokens), 1)
    share = jnp.sum(jnp.where(same, share, 0.0), axis=1, keepdims=True)
    partial = (partial * share).astype(BF16)
    for side, side_ref in enumerate((keep_ref, give_ref)):
        for group in range(groups):
            first = (side * groups + group) * half
            for index in range(pieces):
                side_ref[group * pieces + index] = partial[
                    first : first + half, index * piece : (index + 1) * piece
                ]


def pair_kernel(keep_ref, taken_ref, out_ref):
    out_ref[...] = (keep_ref[...].astype(F32) + taken_ref[...].astype(F32)).astype(BF16)


def finish_kernel(parts_ref, mixed_ref, out_ref):
    half = parts_ref.shape[1]
    for core in range(2):
        mine = slice(core * half, (core + 1) * half)
        total = mixed_ref[...].astype(F32)[mine]
        for index in range(core, parts_ref.shape[0], 2):
            total = total + parts_ref[index].astype(F32)
        out_ref[mine, :] = total.astype(BF16)


def shards(
    stream,
    norm_gain_attn,
    w_query,
    w_key,
    w_value,
    w_forget,
    forget_bias,
    key_cache,
    value_cache,
    gate_cache,
    lengths,
    w_output,
    norm_gain_ffn,
    routes,
    route_weights,
    w_expert_gate,
    w_expert_up,
    expert_down_weight,
):
    count, model_width = stream.shape
    groups = lax.axis_size("ep")
    pieces = lax.axis_size("tp")
    piece = model_width // pieces
    width = key_cache.shape[2]
    shape = jax.ShapeDtypeStruct
    in_vmem = pl.BlockSpec(memory_space=pltpu.VMEM)
    in_smem = pl.BlockSpec(memory_space=pltpu.SMEM)

    paired = groups in (2, 4)
    normed, *blocks = call(
        functools.partial(norm_kernel, paired=paired),
        "norm",
        2 * MIB,
        [shape(stream.shape, BF16)] + [shape((count, model_width // groups), BF16)] * groups,
        flops=COVER,
        in_specs=[pl.BlockSpec(memory_space=pltpu.HBM)] * 2,
        scratch_shapes=[
            pltpu.VMEM(stream.shape, BF16),
            pltpu.VMEM((1, model_width), F32),
            pltpu.SemaphoreType.DMA((2,)),
        ],
    )(
        pltpu.with_memory_space_constraint(stream, pltpu.HBM),
        pltpu.with_memory_space_constraint(norm_gain_attn.reshape(1, -1), pltpu.HBM),
    )
    blocks = exchange(blocks, "ep", paired)
    parts = call(
        project_kernel, "project", 4 * MIB, [shape((count, 3 * width), F32)] * groups
    )(*blocks, w_query, w_key, w_value)
    parts = exchange(parts, "ep", paired)
    outputs = call(
        attend_kernel,
        "attend",
        4 * MIB,
        shape((pieces, count, piece), BF16),
        in_specs=[in_smem] + [in_vmem] * (7 + groups),
        scratch_shapes=[pltpu.VMEM((count, width), F32)],
    )(
        lengths,
        normed,
        w_forget.T,
        forget_bias.reshape(1, -1),
        gate_cache,
        w_output,
        key_cache,
        value_cache,
        *parts,
    )
    head_parts = lax.all_to_all(outputs, "tp", 0, 0, tiled=True)
    half = count // 2
    everyone = ("ep", "tp")
    slots = groups * pieces
    swap = [(one, one ^ 1) for one in range(pieces)]
    mixed, copies = call(
        mix_kernel,
        "mix",
        4 * MIB,
        (shape((count, piece), BF16), shape((slots, half, piece), BF16)),
    )(head_parts, stream)
    near = lax.all_to_all(copies, everyone, 0, 0, tiled=True)
    far = lax.ppermute(near, "tp", swap)
    keep, give = call(
        expert_kernel,
        "experts",
        8 * MIB,
        [shape((slots, half, piece), BF16)] * 2,
        scratch_shapes=[pltpu.VMEM((groups * count, model_width), F32)],
    )(
        near,
        far,
        norm_gain_ffn.reshape(1, -1),
        routes.T,
        route_weights.T,
        jnp.swapaxes(w_expert_gate, 1, 2),
        jnp.swapaxes(w_expert_up, 1, 2),
        expert_down_weight,
    )
    taken = lax.ppermute(give, "tp", swap)
    summed = call(pair_kernel, "pair", 4 * MIB, shape((slots, half, piece), BF16))(keep, taken)
    returned = lax.all_to_all(summed, everyone, 0, 0, tiled=True)
    return call(finish_kernel, "finish", 4 * MIB, shape((count, piece), BF16))(returned, mixed)


def solution(mesh):
    placed = (
        P("ep", None),
        P(),
        P("ep", "tp"),
        P("ep", "tp"),
        P("ep", "tp"),
        P(),
        P(),
        P("ep", None, "tp"),
        P("ep", None, "tp"),
        P("ep", "tp", None),
        P("ep"),
        P("tp", None),
        P(),
        P(),
        P(),
        P("ep", None, "tp"),
        P("ep", None, "tp"),
        P("ep", "tp", None),
    )
    return jax.shard_map(
        shards, mesh=mesh, in_specs=placed, out_specs=P("ep", "tp"), check_vma=False
    )
```

```python
import functools

import jax
import jax.numpy as jnp
from jax import lax
from jax.experimental import pallas as pl
from jax.experimental.pallas import tpu as pltpu
from jax.sharding import PartitionSpec as P

F32 = jnp.float32
BF16 = jnp.bfloat16
ROWS = 8
HIDDEN = -1e30
MIB = 1 << 20
COVER = 40_000_000_000


def call(kernel, name, vmem, outs, flops=0, **options):
    return pl.pallas_call(
        kernel,
        out_shape=outs,
        name=name,
        cost_estimate=pl.CostEstimate(flops=flops, transcendentals=0, bytes_accessed=0),
        compiler_params=pltpu.CompilerParams(vmem_limit_bytes=vmem),
        **options,
    )


def dot_transposed(left, right):
    return lax.dot_general(left, right, (((1,), (1,)), ((), ())), preferred_element_type=F32)


def normalized(floats, gain):
    return floats * lax.rsqrt(jnp.mean(floats * floats, axis=-1, keepdims=True) + 1e-06) * gain


def exchange(items, axis, paired, stride=1):
    size = len(items)
    if paired:
        return [items[0]] + [
            lax.ppermute(
                items[step], axis, [(one, one ^ step * stride) for one in range(size * stride)]
            )
            for step in range(1, size)
        ]
    members = [list(range(first, size * stride, stride)) for first in range(stride)]
    received = lax.all_to_all(
        jnp.stack(items), axis, 0, 0, tiled=True, axis_index_groups=members
    )
    return [received[index] for index in range(size)]


def tree_sum(parts):
    while len(parts) > 1:
        parts = [left + right for left, right in zip(parts[::2], parts[1::2], strict=True)]
    return parts[0]


def norm_kernel(stream_hbm, gain_hbm, *refs, paired):
    normed_ref, *out_refs, stream_ref, gain_ref, sems = refs
    copies = [
        pltpu.make_async_copy(stream_hbm, stream_ref, sems.at[0]),
        pltpu.make_async_copy(gain_hbm, gain_ref, sems.at[1]),
    ]
    for copy in copies:
        copy.start()
    for copy in copies:
        copy.wait()
    width = out_refs[0].shape[1]
    normed_ref[...] = normalized(stream_ref[...].astype(F32), gain_ref[...]).astype(BF16)
    for index, out_ref in enumerate(out_refs):
        group = lax.axis_index("ep") ^ index if paired else index
        out_ref[...] = normed_ref[:, pl.ds(pl.multiple_of(group * width, width), width)]


def project_kernel(*refs):
    groups = (len(refs) - 3) // 2
    block_refs, weight_refs, out_refs = refs[:groups], refs[groups:-groups], refs[-groups:]
    count = block_refs[0].shape[0]
    width = weight_refs[0].shape[1]
    rows = jnp.concatenate([block_ref[...] for block_ref in block_refs], axis=0)
    for index, weight_ref in enumerate(weight_refs):
        part = jnp.dot(rows, weight_ref[...], preferred_element_type=F32)
        for group, out_ref in enumerate(out_refs):
            out_ref[:, index * width : (index + 1) * width] = part[
                group * count : (group + 1) * count
            ]


def attend_kernel(
    lengths_ref,
    normed_ref,
    forget_ref,
    bias_ref,
    gates_ref,
    output_ref,
    keys_ref,
    values_ref,
    *refs,
):
    *part_refs, keep_ref, give_ref, attended_ref, product_ref = refs
    count = normed_ref.shape[0]
    heads = gates_ref.shape[1]
    cache_len = gates_ref.shape[2]
    width = keys_ref.shape[2]
    head_dim = width // heads
    scale = head_dim ** (-0.5)

    forget_all = jax.nn.log_sigmoid(
        dot_transposed(normed_ref[...], forget_ref[...]) + bias_ref[...]
    )
    head_ids = lax.broadcasted_iota(jnp.int32, forget_all.shape, 1)
    first_head = lax.axis_index("tp") * heads
    total = part_refs[0][...]
    for part_ref in part_refs[1:]:
        total = total + part_ref[...]
    query = total[:, :width].astype(BF16).astype(F32)
    key_new = total[:, width : 2 * width].astype(BF16).astype(F32)
    value_new = total[:, 2 * width :].astype(BF16).astype(F32)
    lanes = lax.broadcasted_iota(jnp.int32, (ROWS, width), 1)
    row_ids = lax.broadcasted_iota(jnp.int32, (ROWS, 1), 0)
    positions = lax.broadcasted_iota(jnp.int32, (ROWS, cache_len), 1)

    for first in range(0, count, ROWS):
        mine = slice(first, first + ROWS)
        length = jnp.zeros((ROWS, 1), jnp.int32)
        for row in range(ROWS):
            length = jnp.where(row_ids == row, lengths_ref[first + row], length)
        stacked = jnp.concatenate(
            [
                jnp.where(lanes // head_dim == head, query[mine], 0.0).astype(BF16)
                for head in range(heads)
            ],
            axis=0,
        )
        scores = [jnp.zeros((ROWS, cache_len), F32) for _ in range(heads)]
        for row in range(ROWS):
            products = dot_transposed(stacked, keys_ref[first + row])
            for head in range(heads):
                scores[head] = jnp.where(
                    row_ids == row, products[head * ROWS : (head + 1) * ROWS], scores[head]
                )
        weights = []
        owns = []
        for head in range(heads):
            gates = gates_ref[mine, head, :]
            columns = slice(head * head_dim, (head + 1) * head_dim)
            last_gate = jnp.sum(
                jnp.where(positions == length - 1, gates, 0.0), axis=1, keepdims=True
            )
            forget_new = jnp.sum(
                jnp.where(head_ids[mine] == first_head + head, forget_all[mine], 0.0),
                axis=1,
                keepdims=True,
            )
            own_score = (
                jnp.sum(query[mine, columns] * key_new[mine, columns], axis=1, keepdims=True)
                * scale
            )
            score = scores[head] * scale + forget_new + last_gate - gates
            score = jnp.where(positions < length, score, HIDDEN)
            largest = jnp.maximum(jnp.max(score, axis=1, keepdims=True), own_score)
            past = jnp.exp(score - largest)
            own_term = jnp.exp(own_score - largest)
            norm = jnp.sum(past, axis=1, keepdims=True) + own_term
            weights.append((past / norm).astype(BF16))
            owns.append((own_term / norm).astype(BF16).astype(F32))
        weights = jnp.concatenate(weights, axis=0)
        results = [
            owns[head] * value_new[mine, head * head_dim : (head + 1) * head_dim]
            for head in range(heads)
        ]
        for row in range(ROWS):
            products = jnp.dot(weights, values_ref[first + row], preferred_element_type=F32)
            for head in range(heads):
                columns = slice(head * head_dim, (head + 1) * head_dim)
                results[head] = results[head] + jnp.where(
                    row_ids == row, products[head * ROWS : (head + 1) * ROWS, columns], 0.0
                )
        for head in range(heads):
            attended_ref[mine, head * head_dim : (head + 1) * head_dim] = results[head]

    attended = attended_ref[...].astype(BF16)
    half = keep_ref.shape[1]
    core = lax.axis_index("tp") % 2
    product_ref[...] = jnp.dot(attended, output_ref[...], preferred_element_type=F32)
    keep_ref[...] = product_ref[:, pl.ds(pl.multiple_of(core * half, half), half)]
    give_ref[...] = product_ref[:, pl.ds(pl.multiple_of((1 - core) * half, half), half)].astype(
        BF16
    )


def pair_kernel(keep_ref, taken_ref, out_ref):
    out_ref[...] = (keep_ref[...].astype(F32) + taken_ref[...].astype(F32)).astype(BF16)


def mix_kernel(stream_ref, *refs):
    *part_refs, out_ref = refs
    half = out_ref.shape[1]
    total = tree_sum([part_ref[...].astype(F32) for part_ref in part_refs])
    mine = pl.ds(pl.multiple_of(lax.axis_index("tp") % 2 * half, half), half)
    out_ref[...] = (stream_ref[:, mine].astype(F32) + total).astype(BF16)


def second_norm_kernel(near_ref, far_ref, gain_ref, normed_ref, mixed_ref, row_ref):
    half = near_ref.shape[1]
    piece = mixed_ref.shape[1]
    place = lax.axis_index("tp")
    row_ref[:, pl.ds(pl.multiple_of(place % 2 * half, half), half)] = near_ref[...].astype(F32)
    row_ref[:, pl.ds(pl.multiple_of((1 - place % 2) * half, half), half)] = far_ref[...].astype(
        F32
    )
    normed_ref[...] = normalized(row_ref[...], gain_ref[...]).astype(BF16)
    mixed_ref[...] = row_ref[:, pl.ds(pl.multiple_of(place * piece, piece), piece)].astype(BF16)


def expert_kernel(
    routes_ref, weights_ref, gate_ref, up_ref, down_ref, *refs, groups, paired
):
    row_refs, (keep_ref, give_ref) = refs[:groups], refs[groups:]
    count = row_refs[0].shape[0]
    piece = keep_ref.shape[2]
    pieces = keep_ref.shape[0] // groups
    half = count // 2
    expert = lax.axis_index("ep")
    rows = jnp.concatenate([row_ref[...] for row_ref in row_refs], axis=0)
    gated = dot_transposed(rows, gate_ref[0])
    upper = dot_transposed(rows, up_ref[0])
    hidden = (gated / (1.0 + jnp.exp(-gated)) * upper).astype(BF16)
    partial = jnp.dot(hidden, down_ref[0], preferred_element_type=F32)
    share = jnp.sum(jnp.where(routes_ref[...] == expert, weights_ref[...], 0.0), axis=0, keepdims=True)
    square = (groups * count, groups * count)
    row = lax.broadcasted_iota(jnp.int32, square, 0)
    group = row // count ^ expert if paired else row // count
    same = group * count + row % count == lax.broadcasted_iota(jnp.int32, square, 1)
    share = jnp.sum(jnp.where(same, share, 0.0), axis=1, keepdims=True)
    partial = partial * share
    first_core = lax.axis_index("tp") % 2 == 0
    for index in range(groups):
        lower = partial[index * count : index * count + half]
        upper = partial[index * count + half : (index + 1) * count]
        keep = jnp.where(first_core, lower, upper).astype(BF16)
        give = jnp.where(first_core, upper, lower).astype(BF16)
        group = expert ^ index if paired else index
        for step in range(pieces):
            columns = slice(step * piece, (step + 1) * piece)
            keep_ref[group * pieces + step] = keep[:, columns]
            give_ref[group * pieces + step] = give[:, columns]


def finish_kernel(parts_ref, mixed_ref, out_ref):
    half = parts_ref.shape[1]
    for core in range(2):
        mine = slice(core * half, (core + 1) * half)
        total = mixed_ref[...].astype(F32)[mine]
        for index in range(core, parts_ref.shape[0], 2):
            total = total + parts_ref[index].astype(F32)
        out_ref[mine, :] = total.astype(BF16)


def shards(
    stream,
    norm_gain_attn,
    w_query,
    w_key,
    w_value,
    w_forget,
    forget_bias,
    key_cache,
    value_cache,
    gate_cache,
    lengths,
    w_output,
    norm_gain_ffn,
    routes,
    route_weights,
    w_expert_gate,
    w_expert_up,
    expert_down_weight,
):
    count, model_width = stream.shape
    groups = lax.axis_size("ep")
    pieces = lax.axis_size("tp")
    piece = model_width // pieces
    width = key_cache.shape[2]
    shape = jax.ShapeDtypeStruct
    in_vmem = pl.BlockSpec(memory_space=pltpu.VMEM)
    in_smem = pl.BlockSpec(memory_space=pltpu.SMEM)

    paired = groups in (2, 4)
    normed, *blocks = call(
        functools.partial(norm_kernel, paired=paired),
        "norm",
        2 * MIB,
        [shape(stream.shape, BF16)] + [shape((count, model_width // groups), BF16)] * groups,
        flops=COVER,
        in_specs=[pl.BlockSpec(memory_space=pltpu.HBM)] * 2,
        scratch_shapes=[
            pltpu.VMEM(stream.shape, BF16),
            pltpu.VMEM((1, model_width), F32),
            pltpu.SemaphoreType.DMA((2,)),
        ],
    )(
        pltpu.with_memory_space_constraint(stream, pltpu.HBM),
        pltpu.with_memory_space_constraint(norm_gain_attn.reshape(1, -1), pltpu.HBM),
    )
    blocks = exchange(blocks, "ep", paired)
    parts = call(
        project_kernel, "project", 4 * MIB, [shape((count, 3 * width), F32)] * groups
    )(*blocks, w_query, w_key, w_value)
    parts = exchange(parts, "ep", paired)
    swap = [(one, one ^ 1) for one in range(pieces)]
    side = shape((count, model_width // 2), BF16)
    keep, give = call(
        attend_kernel,
        "attend",
        4 * MIB,
        [shape(side.shape, F32), side],
        in_specs=[in_smem] + [in_vmem] * (7 + groups),
        scratch_shapes=[pltpu.VMEM((count, width), F32), pltpu.VMEM((count, model_width), F32)],
    )(
        lengths,
        normed,
        w_forget.T,
        forget_bias.reshape(1, -1),
        gate_cache,
        w_output,
        key_cache,
        value_cache,
        *parts,
    )
    taken = lax.ppermute(give, "tp", swap)
    pair = call(pair_kernel, "pair", MIB, side)(keep, taken)
    chips = pieces // 2
    pair_parts = exchange([pair] * chips, "tp", chips in (2, 4), 2)
    near = call(mix_kernel, "mix", 2 * MIB, side)(stream, *pair_parts)
    far = lax.ppermute(near, "tp", swap)
    rows, mixed = call(
        second_norm_kernel,
        "second_norm",
        2 * MIB,
        [shape(stream.shape, BF16), shape((count, piece), BF16)],
        scratch_shapes=[pltpu.VMEM(stream.shape, F32)],
    )(near, far, norm_gain_ffn.reshape(1, -1))
    half = count // 2
    slots = groups * pieces
    keep, give = call(
        functools.partial(expert_kernel, groups=groups, paired=paired),
        "experts",
        8 * MIB,
        [shape((slots, half, piece), BF16)] * 2,
    )(
        routes.T,
        route_weights.T,
        jnp.swapaxes(w_expert_gate, 1, 2),
        jnp.swapaxes(w_expert_up, 1, 2),
        expert_down_weight,
        *exchange([rows] * groups, "ep", paired),
    )
    taken = lax.ppermute(give, "tp", swap)
    summed = call(pair_kernel, "sides", 4 * MIB, shape((slots, half, piece), BF16))(keep, taken)
    returned = lax.all_to_all(summed, ("ep", "tp"), 0, 0, tiled=True)
    return call(finish_kernel, "finish", 4 * MIB, shape((count, piece), BF16))(returned, mixed)


def solution(mesh):
    placed = (
        P("ep", None),
        P(),
        P("ep", "tp"),
        P("ep", "tp"),
        P("ep", "tp"),
        P(),
        P(),
        P("ep", None, "tp"),
        P("ep", None, "tp"),
        P("ep", "tp", None),
        P("ep"),
        P("tp", None),
        P(),
        P(),
        P(),
        P("ep", None, "tp"),
        P("ep", None, "tp"),
        P("ep", "tp", None),
    )
    return jax.shard_map(
        shards, mesh=mesh, in_specs=placed, out_specs=P("ep", "tp"), check_vma=False
    )
```

```python
import functools

import jax
import jax.numpy as jnp
from jax import lax
from jax.experimental import pallas as pl
from jax.experimental.pallas import tpu as pltpu
from jax.sharding import PartitionSpec as P

F32 = jnp.float32
BF16 = jnp.bfloat16
ROWS = 8
BLOCK = 256
HIDDEN = -1e30
MIB = 1 << 20
COVER = 40_000_000_000


def call(kernel, name, vmem, outs, flops=0, **options):
    return pl.pallas_call(
        kernel,
        out_shape=outs,
        name=name,
        cost_estimate=pl.CostEstimate(flops=flops, transcendentals=0, bytes_accessed=0),
        compiler_params=pltpu.CompilerParams(vmem_limit_bytes=vmem),
        **options,
    )


def dot_transposed(left, right):
    return lax.dot_general(left, right, (((1,), (1,)), ((), ())), preferred_element_type=F32)


def normalized(floats, gain):
    return floats * lax.rsqrt(jnp.mean(floats * floats, axis=-1, keepdims=True) + 1e-06) * gain


def exchange(items, axis, paired, stride=1):
    size = len(items)
    if paired:
        return [items[0]] + [
            lax.ppermute(
                items[step], axis, [(one, one ^ step * stride) for one in range(size * stride)]
            )
            for step in range(1, size)
        ]
    members = [list(range(first, size * stride, stride)) for first in range(stride)]
    received = lax.all_to_all(
        jnp.stack(items), axis, 0, 0, tiled=True, axis_index_groups=members
    )
    return [received[index] for index in range(size)]


def tree_sum(parts):
    while len(parts) > 1:
        parts = [left + right for left, right in zip(parts[::2], parts[1::2], strict=True)]
    return parts[0]


def norm_kernel(stream_hbm, gain_hbm, *refs, paired):
    normed_ref, *out_refs, stream_ref, gain_ref, sems = refs
    copies = [
        pltpu.make_async_copy(stream_hbm, stream_ref, sems.at[0]),
        pltpu.make_async_copy(gain_hbm, gain_ref, sems.at[1]),
    ]
    for copy in copies:
        copy.start()
    for copy in copies:
        copy.wait()
    width = out_refs[0].shape[1]
    normed_ref[...] = normalized(stream_ref[...].astype(F32), gain_ref[...]).astype(BF16)
    for index, out_ref in enumerate(out_refs):
        group = lax.axis_index("ep") ^ index if paired else index
        out_ref[...] = normed_ref[:, pl.ds(pl.multiple_of(group * width, width), width)]


def project_kernel(*refs):
    groups = (len(refs) - 3) // 2
    block_refs, weight_refs, out_refs = refs[:groups], refs[groups:-groups], refs[-groups:]
    count = block_refs[0].shape[0]
    width = weight_refs[0].shape[1]
    rows = jnp.concatenate([block_ref[...] for block_ref in block_refs], axis=0)
    for index, weight_ref in enumerate(weight_refs):
        part = jnp.dot(rows, weight_ref[...], preferred_element_type=F32)
        for group, out_ref in enumerate(out_refs):
            out_ref[:, index * width : (index + 1) * width] = part[
                group * count : (group + 1) * count
            ]


def attend_kernel(
    lengths_ref,
    normed_ref,
    forget_ref,
    bias_ref,
    gates_ref,
    output_ref,
    keys_ref,
    values_ref,
    *refs,
):
    *part_refs, keep_ref, give_ref, attended_ref, product_ref, scores_ref = refs
    count = normed_ref.shape[0]
    heads = gates_ref.shape[1]
    cache_len = gates_ref.shape[2]
    width = keys_ref.shape[2]
    head_dim = width // heads
    scale = head_dim ** (-0.5)

    forget_all = jax.nn.log_sigmoid(
        dot_transposed(normed_ref[...], forget_ref[...]) + bias_ref[...]
    )
    head_ids = lax.broadcasted_iota(jnp.int32, forget_all.shape, 1)
    first_head = lax.axis_index("tp") * heads
    total = part_refs[0][...]
    for part_ref in part_refs[1:]:
        total = total + part_ref[...]
    query = total[:, :width].astype(BF16).astype(F32)
    key_new = total[:, width : 2 * width].astype(BF16).astype(F32)
    value_new = total[:, 2 * width :].astype(BF16).astype(F32)
    lanes = lax.broadcasted_iota(jnp.int32, (ROWS, width), 1)
    row_ids = lax.broadcasted_iota(jnp.int32, (ROWS, 1), 0)
    positions = lax.broadcasted_iota(jnp.int32, (ROWS, cache_len), 1)

    def stacked(first):
        return jnp.concatenate(
            [
                jnp.where(lanes // head_dim == head, query[first : first + ROWS], 0.0).astype(BF16)
                for head in range(heads)
            ],
            axis=0,
        )

    for pair in range(0, count, 2 * ROWS):
        streamed, loaded = stacked(pair), stacked(pair + ROWS)
        lane_row = lax.broadcasted_iota(jnp.int32, (BLOCK, heads * ROWS), 1) % ROWS
        loaded_row = lax.broadcasted_iota(jnp.int32, (heads * ROWS, BLOCK), 0) % ROWS
        for start in range(0, cache_len, BLOCK):
            block = slice(start, start + BLOCK)
            down = jnp.zeros((BLOCK, heads * ROWS), F32)
            over = jnp.zeros((heads * ROWS, BLOCK), F32)
            for row in range(ROWS):
                products = dot_transposed(keys_ref[pair + row, block, :], streamed)
                down = jnp.where(lane_row == row, products, down)
                products = dot_transposed(loaded, keys_ref[pair + ROWS + row, block, :])
                over = jnp.where(loaded_row == row, products, over)
            base = heads * pair
            scores_ref[base : base + heads * ROWS, block] = down.T
            scores_ref[base + heads * ROWS : base + 2 * heads * ROWS, block] = over

    for first in range(0, count, ROWS):
        mine = slice(first, first + ROWS)
        length = jnp.zeros((ROWS, 1), jnp.int32)
        for row in range(ROWS):
            length = jnp.where(row_ids == row, lengths_ref[first + row], length)
        base = heads * first
        scores = [
            scores_ref[base + head * ROWS : base + (head + 1) * ROWS, :] for head in range(heads)
        ]
        weights = []
        owns = []
        for head in range(heads):
            gates = gates_ref[mine, head, :]
            columns = slice(head * head_dim, (head + 1) * head_dim)
            last_gate = jnp.sum(
                jnp.where(positions == length - 1, gates, 0.0), axis=1, keepdims=True
            )
            forget_new = jnp.sum(
                jnp.where(head_ids[mine] == first_head + head, forget_all[mine], 0.0),
                axis=1,
                keepdims=True,
            )
            own_score = (
                jnp.sum(query[mine, columns] * key_new[mine, columns], axis=1, keepdims=True)
                * scale
            )
            score = scores[head] * scale + forget_new + last_gate - gates
            score = jnp.where(positions < length, score, HIDDEN)
            largest = jnp.maximum(jnp.max(score, axis=1, keepdims=True), own_score)
            past = jnp.exp(score - largest)
            own_term = jnp.exp(own_score - largest)
            norm = jnp.sum(past, axis=1, keepdims=True) + own_term
            weights.append((past / norm).astype(BF16))
            owns.append((own_term / norm).astype(BF16).astype(F32))
        weights = jnp.concatenate(weights, axis=0)
        results = [
            owns[head] * value_new[mine, head * head_dim : (head + 1) * head_dim]
            for head in range(heads)
        ]
        for row in range(ROWS):
            products = jnp.dot(weights, values_ref[first + row], preferred_element_type=F32)
            for head in range(heads):
                columns = slice(head * head_dim, (head + 1) * head_dim)
                results[head] = results[head] + jnp.where(
                    row_ids == row, products[head * ROWS : (head + 1) * ROWS, columns], 0.0
                )
        for head in range(heads):
            attended_ref[mine, head * head_dim : (head + 1) * head_dim] = results[head]

    attended = attended_ref[...].astype(BF16)
    half = keep_ref.shape[1]
    core = lax.axis_index("tp") % 2
    product_ref[...] = jnp.dot(attended, output_ref[...], preferred_element_type=F32)
    keep_ref[...] = product_ref[:, pl.ds(pl.multiple_of(core * half, half), half)]
    give_ref[...] = product_ref[:, pl.ds(pl.multiple_of((1 - core) * half, half), half)].astype(
        BF16
    )


def pair_kernel(keep_ref, taken_ref, out_ref):
    out_ref[...] = (keep_ref[...].astype(F32) + taken_ref[...].astype(F32)).astype(BF16)


def mix_kernel(stream_ref, *refs):
    *part_refs, out_ref = refs
    half = out_ref.shape[1]
    total = tree_sum([part_ref[...].astype(F32) for part_ref in part_refs])
    mine = pl.ds(pl.multiple_of(lax.axis_index("tp") % 2 * half, half), half)
    out_ref[...] = (stream_ref[:, mine].astype(F32) + total).astype(BF16)


def second_norm_kernel(near_ref, far_ref, gain_ref, normed_ref, mixed_ref, row_ref):
    half = near_ref.shape[1]
    piece = mixed_ref.shape[1]
    place = lax.axis_index("tp")
    row_ref[:, pl.ds(pl.multiple_of(place % 2 * half, half), half)] = near_ref[...].astype(F32)
    row_ref[:, pl.ds(pl.multiple_of((1 - place % 2) * half, half), half)] = far_ref[...].astype(
        F32
    )
    normed_ref[...] = normalized(row_ref[...], gain_ref[...]).astype(BF16)
    mixed_ref[...] = row_ref[:, pl.ds(pl.multiple_of(place * piece, piece), piece)].astype(BF16)


def expert_kernel(
    routes_ref, weights_ref, gate_ref, up_ref, down_ref, *refs, groups, paired
):
    row_refs, (keep_ref, give_ref) = refs[:groups], refs[groups:]
    count = row_refs[0].shape[0]
    piece = keep_ref.shape[2]
    pieces = keep_ref.shape[0] // groups
    half = count // 2
    expert = lax.axis_index("ep")
    rows = jnp.concatenate([row_ref[...] for row_ref in row_refs], axis=0)
    hidden = []
    for start in range(0, gate_ref.shape[1], BLOCK):
        units = slice(start, min(start + BLOCK, gate_ref.shape[1]))
        gated, upper = 0.0, 0.0
        for first in range(0, rows.shape[1], BLOCK):
            features = slice(first, first + BLOCK)
            gated += dot_transposed(rows[:, features], gate_ref[0, units, features])
            upper += dot_transposed(up_ref[0, units, features], rows[:, features])
        hidden.append((gated / (1.0 + jnp.exp(-gated)) * upper.T).astype(BF16))
    hidden = jnp.concatenate(hidden, axis=1)
    partial = jnp.dot(hidden, down_ref[0], preferred_element_type=F32)
    share = jnp.sum(jnp.where(routes_ref[...] == expert, weights_ref[...], 0.0), axis=0, keepdims=True)
    square = (groups * count, groups * count)
    row = lax.broadcasted_iota(jnp.int32, square, 0)
    group = row // count ^ expert if paired else row // count
    same = group * count + row % count == lax.broadcasted_iota(jnp.int32, square, 1)
    share = jnp.sum(jnp.where(same, share, 0.0), axis=1, keepdims=True)
    partial = partial * share
    first_core = lax.axis_index("tp") % 2 == 0
    for index in range(groups):
        lower = partial[index * count : index * count + half]
        upper = partial[index * count + half : (index + 1) * count]
        keep = jnp.where(first_core, lower, upper).astype(BF16)
        give = jnp.where(first_core, upper, lower).astype(BF16)
        group = expert ^ index if paired else index
        for step in range(pieces):
            columns = slice(step * piece, (step + 1) * piece)
            keep_ref[group * pieces + step] = keep[:, columns]
            give_ref[group * pieces + step] = give[:, columns]


def finish_kernel(parts_ref, mixed_ref, out_ref):
    half = parts_ref.shape[1]
    for core in range(2):
        mine = slice(core * half, (core + 1) * half)
        total = mixed_ref[...].astype(F32)[mine]
        for index in range(core, parts_ref.shape[0], 2):
            total = total + parts_ref[index].astype(F32)
        out_ref[mine, :] = total.astype(BF16)


def shards(
    stream,
    norm_gain_attn,
    w_query,
    w_key,
    w_value,
    w_forget,
    forget_bias,
    key_cache,
    value_cache,
    gate_cache,
    lengths,
    w_output,
    norm_gain_ffn,
    routes,
    route_weights,
    w_expert_gate,
    w_expert_up,
    expert_down_weight,
):
    count, model_width = stream.shape
    groups = lax.axis_size("ep")
    pieces = lax.axis_size("tp")
    piece = model_width // pieces
    width = key_cache.shape[2]
    shape = jax.ShapeDtypeStruct
    in_vmem = pl.BlockSpec(memory_space=pltpu.VMEM)
    in_smem = pl.BlockSpec(memory_space=pltpu.SMEM)

    paired = groups in (2, 4)
    normed, *blocks = call(
        functools.partial(norm_kernel, paired=paired),
        "norm",
        2 * MIB,
        [shape(stream.shape, BF16)] + [shape((count, model_width // groups), BF16)] * groups,
        flops=COVER,
        in_specs=[pl.BlockSpec(memory_space=pltpu.HBM)] * 2,
        scratch_shapes=[
            pltpu.VMEM(stream.shape, BF16),
            pltpu.VMEM((1, model_width), F32),
            pltpu.SemaphoreType.DMA((2,)),
        ],
    )(
        pltpu.with_memory_space_constraint(stream, pltpu.HBM),
        pltpu.with_memory_space_constraint(norm_gain_attn.reshape(1, -1), pltpu.HBM),
    )
    blocks = exchange(blocks, "ep", paired)
    parts = call(
        project_kernel, "project", 4 * MIB, [shape((count, 3 * width), F32)] * groups
    )(*blocks, w_query, w_key, w_value)
    parts = exchange(parts, "ep", paired)
    swap = [(one, one ^ 1) for one in range(pieces)]
    side = shape((count, model_width // 2), BF16)
    keep, give = call(
        attend_kernel,
        "attend",
        4 * MIB,
        [shape(side.shape, F32), side],
        in_specs=[in_smem] + [in_vmem] * (7 + groups),
        scratch_shapes=[
            pltpu.VMEM((count, width), F32),
            pltpu.VMEM((count, model_width), F32),
            pltpu.VMEM((gate_cache.shape[1] * count, gate_cache.shape[2]), F32),
        ],
    )(
        lengths,
        normed,
        w_forget.T,
        forget_bias.reshape(1, -1),
        gate_cache,
        w_output,
        key_cache,
        value_cache,
        *parts,
    )
    taken = lax.ppermute(give, "tp", swap)
    pair = call(pair_kernel, "pair", MIB, side)(keep, taken)
    chips = pieces // 2
    pair_parts = exchange([pair] * chips, "tp", chips in (2, 4), 2)
    near = call(mix_kernel, "mix", 2 * MIB, side)(stream, *pair_parts)
    far = lax.ppermute(near, "tp", swap)
    rows, mixed = call(
        second_norm_kernel,
        "second_norm",
        2 * MIB,
        [shape(stream.shape, BF16), shape((count, piece), BF16)],
        scratch_shapes=[pltpu.VMEM(stream.shape, F32)],
    )(near, far, norm_gain_ffn.reshape(1, -1))
    half = count // 2
    slots = groups * pieces
    keep, give = call(
        functools.partial(expert_kernel, groups=groups, paired=paired),
        "experts",
        8 * MIB,
        [shape((slots, half, piece), BF16)] * 2,
    )(
        routes.T,
        route_weights.T,
        jnp.swapaxes(w_expert_gate, 1, 2),
        jnp.swapaxes(w_expert_up, 1, 2),
        expert_down_weight,
        *exchange([rows] * groups, "ep", paired),
    )
    taken = lax.ppermute(give, "tp", swap)
    summed = call(pair_kernel, "sides", 4 * MIB, shape((slots, half, piece), BF16))(keep, taken)
    returned = lax.all_to_all(summed, ("ep", "tp"), 0, 0, tiled=True)
    return call(finish_kernel, "finish", 4 * MIB, shape((count, piece), BF16))(returned, mixed)


def solution(mesh):
    placed = (
        P("ep", None),
        P(),
        P("ep", "tp"),
        P("ep", "tp"),
        P("ep", "tp"),
        P(),
        P(),
        P("ep", None, "tp"),
        P("ep", None, "tp"),
        P("ep", "tp", None),
        P("ep"),
        P("tp", None),
        P(),
        P(),
        P(),
        P("ep", None, "tp"),
        P("ep", None, "tp"),
        P("ep", "tp", None),
    )
    return jax.shard_map(
        shards, mesh=mesh, in_specs=placed, out_specs=P("ep", "tp"), check_vma=False
    )
```

```python
import functools

import jax
import jax.numpy as jnp
from jax import lax
from jax.experimental import pallas as pl
from jax.experimental.pallas import tpu as pltpu
from jax.sharding import PartitionSpec as P

F32 = jnp.float32
BF16 = jnp.bfloat16
ROWS = 8
BLOCK = 256
HIDDEN = -1e30
MIB = 1 << 20
COVER = 40_000_000_000


def call(kernel, name, vmem, outs, flops=0, **options):
    return pl.pallas_call(
        kernel,
        out_shape=outs,
        name=name,
        cost_estimate=pl.CostEstimate(flops=flops, transcendentals=0, bytes_accessed=0),
        compiler_params=pltpu.CompilerParams(vmem_limit_bytes=vmem),
        **options,
    )


def dot_transposed(left, right):
    return lax.dot_general(left, right, (((1,), (1,)), ((), ())), preferred_element_type=F32)


def normalized(floats, gain):
    return floats * lax.rsqrt(jnp.mean(floats * floats, axis=-1, keepdims=True) + 1e-06) * gain


def exchange(items, axis, paired, stride=1, steps=None):
    size = len(items)
    steps = steps or range(size)
    if paired:
        return [items[0]] + [
            lax.ppermute(
                items[index],
                axis,
                [(one, one ^ steps[index] * stride) for one in range(size * stride)],
            )
            for index in range(1, size)
        ]
    members = [list(range(first, size * stride, stride)) for first in range(stride)]
    received = lax.all_to_all(
        jnp.stack(items), axis, 0, 0, tiled=True, axis_index_groups=members
    )
    return [received[index] for index in range(size)]


def tree_sum(parts):
    while len(parts) > 1:
        parts = [left + right for left, right in zip(parts[::2], parts[1::2], strict=True)]
    return parts[0]


def norm_kernel(stream_hbm, gain_hbm, *refs, paired, steps):
    normed_ref, *out_refs, stream_ref, gain_ref, sems = refs
    copies = [
        pltpu.make_async_copy(stream_hbm, stream_ref, sems.at[0]),
        pltpu.make_async_copy(gain_hbm, gain_ref, sems.at[1]),
    ]
    for copy in copies:
        copy.start()
    for copy in copies:
        copy.wait()
    width = out_refs[0].shape[1]
    normed_ref[...] = normalized(stream_ref[...].astype(F32), gain_ref[...]).astype(BF16)
    for index, out_ref in enumerate(out_refs):
        group = lax.axis_index("ep") ^ steps[index] if paired else index
        out_ref[...] = normed_ref[:, pl.ds(pl.multiple_of(group * width, width), width)]


def project_kernel(*refs):
    groups = (len(refs) - 3) // 2
    block_refs, weight_refs, out_refs = refs[:groups], refs[groups:-groups], refs[-groups:]
    count = block_refs[0].shape[0]
    width = weight_refs[0].shape[1]
    rows = jnp.concatenate([block_ref[...] for block_ref in block_refs], axis=0)
    for index, weight_ref in enumerate(weight_refs):
        part = jnp.dot(rows, weight_ref[...], preferred_element_type=F32)
        for group, out_ref in enumerate(out_refs):
            out_ref[:, index * width : (index + 1) * width] = part[
                group * count : (group + 1) * count
            ]


def attend_kernel(
    lengths_ref,
    normed_ref,
    forget_ref,
    bias_ref,
    gates_ref,
    output_ref,
    keys_ref,
    values_ref,
    *refs,
):
    *part_refs, keep_ref, give_ref, attended_ref, product_ref, scores_ref = refs
    count = normed_ref.shape[0]
    heads = gates_ref.shape[1]
    cache_len = gates_ref.shape[2]
    width = keys_ref.shape[2]
    head_dim = width // heads
    scale = head_dim ** (-0.5)

    forget_all = jax.nn.log_sigmoid(
        dot_transposed(normed_ref[...], forget_ref[...]) + bias_ref[...]
    )
    head_ids = lax.broadcasted_iota(jnp.int32, forget_all.shape, 1)
    first_head = lax.axis_index("tp") * heads
    total = part_refs[0][...]
    for part_ref in part_refs[1:]:
        total = total + part_ref[...]
    query = total[:, :width].astype(BF16).astype(F32)
    key_new = total[:, width : 2 * width].astype(BF16).astype(F32)
    value_new = total[:, 2 * width :].astype(BF16).astype(F32)
    lanes = lax.broadcasted_iota(jnp.int32, (ROWS, width), 1)
    row_ids = lax.broadcasted_iota(jnp.int32, (ROWS, 1), 0)
    positions = lax.broadcasted_iota(jnp.int32, (ROWS, cache_len), 1)

    def stacked(first):
        return jnp.concatenate(
            [
                jnp.where(lanes // head_dim == head, query[first : first + ROWS], 0.0).astype(BF16)
                for head in range(heads)
            ],
            axis=0,
        )

    for pair in range(0, count, 2 * ROWS):
        streamed, loaded = stacked(pair), stacked(pair + ROWS)
        lane_row = lax.broadcasted_iota(jnp.int32, (BLOCK, heads * ROWS), 1) % ROWS
        loaded_row = lax.broadcasted_iota(jnp.int32, (heads * ROWS, BLOCK), 0) % ROWS
        for start in range(0, cache_len, BLOCK):
            block = slice(start, start + BLOCK)
            down = jnp.zeros((BLOCK, heads * ROWS), F32)
            over = jnp.zeros((heads * ROWS, BLOCK), F32)
            for row in range(ROWS):
                products = dot_transposed(keys_ref[pair + row, block, :], streamed)
                down = jnp.where(lane_row == row, products, down)
                products = dot_transposed(loaded, keys_ref[pair + ROWS + row, block, :])
                over = jnp.where(loaded_row == row, products, over)
            base = heads * pair
            scores_ref[base : base + heads * ROWS, block] = down.T
            scores_ref[base + heads * ROWS : base + 2 * heads * ROWS, block] = over

    for first in range(0, count, ROWS):
        mine = slice(first, first + ROWS)
        length = jnp.zeros((ROWS, 1), jnp.int32)
        for row in range(ROWS):
            length = jnp.where(row_ids == row, lengths_ref[first + row], length)
        base = heads * first
        scores = [
            scores_ref[base + head * ROWS : base + (head + 1) * ROWS, :] for head in range(heads)
        ]
        weights = []
        owns = []
        for head in range(heads):
            gates = gates_ref[mine, head, :]
            columns = slice(head * head_dim, (head + 1) * head_dim)
            last_gate = jnp.sum(
                jnp.where(positions == length - 1, gates, 0.0), axis=1, keepdims=True
            )
            forget_new = jnp.sum(
                jnp.where(head_ids[mine] == first_head + head, forget_all[mine], 0.0),
                axis=1,
                keepdims=True,
            )
            own_score = (
                jnp.sum(query[mine, columns] * key_new[mine, columns], axis=1, keepdims=True)
                * scale
            )
            score = scores[head] * scale + forget_new + last_gate - gates
            score = jnp.where(positions < length, score, HIDDEN)
            largest = jnp.maximum(jnp.max(score, axis=1, keepdims=True), own_score)
            past = jnp.exp(score - largest)
            own_term = jnp.exp(own_score - largest)
            norm = jnp.sum(past, axis=1, keepdims=True) + own_term
            weights.append((past / norm).astype(BF16))
            owns.append((own_term / norm).astype(BF16).astype(F32))
        weights = jnp.concatenate(weights, axis=0)
        results = [
            owns[head] * value_new[mine, head * head_dim : (head + 1) * head_dim]
            for head in range(heads)
        ]
        for row in range(ROWS):
            products = jnp.dot(weights, values_ref[first + row], preferred_element_type=F32)
            for head in range(heads):
                columns = slice(head * head_dim, (head + 1) * head_dim)
                results[head] = results[head] + jnp.where(
                    row_ids == row, products[head * ROWS : (head + 1) * ROWS, columns], 0.0
                )
        for head in range(heads):
            attended_ref[mine, head * head_dim : (head + 1) * head_dim] = results[head]

    attended = attended_ref[...].astype(BF16)
    half = keep_ref.shape[1]
    core = lax.axis_index("tp") % 2
    product_ref[...] = jnp.dot(attended, output_ref[...], preferred_element_type=F32)
    keep_ref[...] = product_ref[:, pl.ds(pl.multiple_of(core * half, half), half)]
    give_ref[...] = product_ref[:, pl.ds(pl.multiple_of((1 - core) * half, half), half)].astype(
        BF16
    )


def pair_kernel(keep_ref, taken_ref, out_ref):
    out_ref[...] = (keep_ref[...].astype(F32) + taken_ref[...].astype(F32)).astype(BF16)


def mix_kernel(stream_ref, *refs):
    *part_refs, out_ref = refs
    half = out_ref.shape[1]
    total = tree_sum([part_ref[...].astype(F32) for part_ref in part_refs])
    mine = pl.ds(pl.multiple_of(lax.axis_index("tp") % 2 * half, half), half)
    out_ref[...] = (stream_ref[:, mine].astype(F32) + total).astype(BF16)


def second_norm_kernel(near_ref, far_ref, gain_ref, normed_ref, mixed_ref, row_ref):
    half = near_ref.shape[1]
    piece = mixed_ref.shape[1]
    place = lax.axis_index("tp")
    row_ref[:, pl.ds(pl.multiple_of(place % 2 * half, half), half)] = near_ref[...].astype(F32)
    row_ref[:, pl.ds(pl.multiple_of((1 - place % 2) * half, half), half)] = far_ref[...].astype(
        F32
    )
    normed_ref[...] = normalized(row_ref[...], gain_ref[...]).astype(BF16)
    mixed_ref[...] = row_ref[:, pl.ds(pl.multiple_of(place * piece, piece), piece)].astype(BF16)


def expert_kernel(
    routes_ref, weights_ref, gate_ref, up_ref, down_ref, *refs, groups, paired
):
    row_refs, (keep_ref, give_ref) = refs[:groups], refs[groups:]
    count = row_refs[0].shape[0]
    piece = keep_ref.shape[2]
    pieces = keep_ref.shape[0] // groups
    half = count // 2
    expert = lax.axis_index("ep")
    rows = jnp.concatenate([row_ref[...] for row_ref in row_refs], axis=0)
    hidden = []
    for start in range(0, gate_ref.shape[1], BLOCK):
        units = slice(start, min(start + BLOCK, gate_ref.shape[1]))
        gated, upper = 0.0, 0.0
        for first in range(0, rows.shape[1], BLOCK):
            features = slice(first, first + BLOCK)
            gated += dot_transposed(rows[:, features], gate_ref[0, units, features])
            upper += dot_transposed(up_ref[0, units, features], rows[:, features])
        hidden.append((gated / (1.0 + jnp.exp(-gated)) * upper.T).astype(BF16))
    hidden = jnp.concatenate(hidden, axis=1)
    partial = jnp.dot(hidden, down_ref[0], preferred_element_type=F32)
    share = jnp.sum(jnp.where(routes_ref[...] == expert, weights_ref[...], 0.0), axis=0, keepdims=True)
    square = (groups * count, groups * count)
    row = lax.broadcasted_iota(jnp.int32, square, 0)
    group = row // count ^ expert if paired else row // count
    same = group * count + row % count == lax.broadcasted_iota(jnp.int32, square, 1)
    share = jnp.sum(jnp.where(same, share, 0.0), axis=1, keepdims=True)
    partial = partial * share
    first_core = lax.axis_index("tp") % 2 == 0
    for index in range(groups):
        lower = partial[index * count : index * count + half]
        upper = partial[index * count + half : (index + 1) * count]
        keep = jnp.where(first_core, lower, upper).astype(BF16)
        give = jnp.where(first_core, upper, lower).astype(BF16)
        group = expert ^ index if paired else index
        for step in range(pieces):
            columns = slice(step * piece, (step + 1) * piece)
            keep_ref[group * pieces + step] = keep[:, columns]
            give_ref[group * pieces + step] = give[:, columns]


def finish_kernel(parts_ref, mixed_ref, out_ref):
    half = parts_ref.shape[1]
    for core in range(2):
        mine = slice(core * half, (core + 1) * half)
        total = mixed_ref[...].astype(F32)[mine]
        for index in range(core, parts_ref.shape[0], 2):
            total = total + parts_ref[index].astype(F32)
        out_ref[mine, :] = total.astype(BF16)


def shards(
    stream,
    norm_gain_attn,
    w_query,
    w_key,
    w_value,
    w_forget,
    forget_bias,
    key_cache,
    value_cache,
    gate_cache,
    lengths,
    w_output,
    norm_gain_ffn,
    routes,
    route_weights,
    w_expert_gate,
    w_expert_up,
    expert_down_weight,
):
    count, model_width = stream.shape
    groups = lax.axis_size("ep")
    pieces = lax.axis_size("tp")
    piece = model_width // pieces
    width = key_cache.shape[2]
    shape = jax.ShapeDtypeStruct
    in_vmem = pl.BlockSpec(memory_space=pltpu.VMEM)
    in_smem = pl.BlockSpec(memory_space=pltpu.SMEM)

    paired = groups in (2, 4)
    steps = (0, 3, 1, 2) if groups == 4 else tuple(range(groups))
    normed, *blocks = call(
        functools.partial(norm_kernel, paired=paired, steps=steps),
        "norm",
        2 * MIB,
        [shape(stream.shape, BF16)] + [shape((count, model_width // groups), BF16)] * groups,
        flops=COVER,
        in_specs=[pl.BlockSpec(memory_space=pltpu.HBM)] * 2,
        scratch_shapes=[
            pltpu.VMEM(stream.shape, BF16),
            pltpu.VMEM((1, model_width), F32),
            pltpu.SemaphoreType.DMA((2,)),
        ],
    )(
        pltpu.with_memory_space_constraint(stream, pltpu.HBM),
        pltpu.with_memory_space_constraint(norm_gain_attn.reshape(1, -1), pltpu.HBM),
    )
    blocks = exchange(blocks, "ep", paired, steps=steps)
    parts = call(
        project_kernel, "project", 4 * MIB, [shape((count, 3 * width), F32)] * groups
    )(*blocks, w_query, w_key, w_value)
    parts = exchange(parts, "ep", paired, steps=steps)
    swap = [(one, one ^ 1) for one in range(pieces)]
    side = shape((count, model_width // 2), BF16)
    keep, give = call(
        attend_kernel,
        "attend",
        4 * MIB,
        [shape(side.shape, F32), side],
        in_specs=[in_smem] + [in_vmem] * (7 + groups),
        scratch_shapes=[
            pltpu.VMEM((count, width), F32),
            pltpu.VMEM((count, model_width), F32),
            pltpu.VMEM((gate_cache.shape[1] * count, gate_cache.shape[2]), F32),
        ],
    )(
        lengths,
        normed,
        w_forget.T,
        forget_bias.reshape(1, -1),
        gate_cache,
        w_output,
        key_cache,
        value_cache,
        *parts,
    )
    taken = lax.ppermute(give, "tp", swap)
    pair = call(pair_kernel, "pair", MIB, side)(keep, taken)
    chips = pieces // 2
    pair_parts = exchange([pair] * chips, "tp", chips in (2, 4), 2)
    near = call(mix_kernel, "mix", 2 * MIB, side)(stream, *pair_parts)
    far = lax.ppermute(near, "tp", swap)
    rows, mixed = call(
        second_norm_kernel,
        "second_norm",
        2 * MIB,
        [shape(stream.shape, BF16), shape((count, piece), BF16)],
        scratch_shapes=[pltpu.VMEM(stream.shape, F32)],
    )(near, far, norm_gain_ffn.reshape(1, -1))
    half = count // 2
    slots = groups * pieces
    keep, give = call(
        functools.partial(expert_kernel, groups=groups, paired=paired),
        "experts",
        8 * MIB,
        [shape((slots, half, piece), BF16)] * 2,
    )(
        routes.T,
        route_weights.T,
        jnp.swapaxes(w_expert_gate, 1, 2),
        jnp.swapaxes(w_expert_up, 1, 2),
        expert_down_weight,
        *exchange([rows] * groups, "ep", paired),
    )
    taken = lax.ppermute(give, "tp", swap)
    summed = call(pair_kernel, "sides", 4 * MIB, shape((slots, half, piece), BF16))(keep, taken)
    returned = lax.all_to_all(summed, ("ep", "tp"), 0, 0, tiled=True)
    return call(finish_kernel, "finish", 4 * MIB, shape((count, piece), BF16))(returned, mixed)


def solution(mesh):
    placed = (
        P("ep", None),
        P(),
        P("ep", "tp"),
        P("ep", "tp"),
        P("ep", "tp"),
        P(),
        P(),
        P("ep", None, "tp"),
        P("ep", None, "tp"),
        P("ep", "tp", None),
        P("ep"),
        P("tp", None),
        P(),
        P(),
        P(),
        P("ep", None, "tp"),
        P("ep", None, "tp"),
        P("ep", "tp", None),
    )
    return jax.shard_map(
        shards, mesh=mesh, in_specs=placed, out_specs=P("ep", "tp"), check_vma=False
    )
```

```python
import functools

import jax
import jax.numpy as jnp
from jax import lax
from jax.experimental import pallas as pl
from jax.experimental.pallas import tpu as pltpu
from jax.sharding import PartitionSpec as P

F32 = jnp.float32
BF16 = jnp.bfloat16
ROWS = 8
BLOCK = 256
HIDDEN = -1e30
MIB = 1 << 20
COVER = 40_000_000_000


def call(kernel, name, vmem, outs, flops=0, **options):
    return pl.pallas_call(
        kernel,
        out_shape=outs,
        name=name,
        cost_estimate=pl.CostEstimate(flops=flops, transcendentals=0, bytes_accessed=0),
        compiler_params=pltpu.CompilerParams(vmem_limit_bytes=vmem),
        **options,
    )


def dot_transposed(left, right):
    return lax.dot_general(left, right, (((1,), (1,)), ((), ())), preferred_element_type=F32)


def normalized(floats, gain):
    return floats * lax.rsqrt(jnp.mean(floats * floats, axis=-1, keepdims=True) + 1e-06) * gain


def exchange(items, axis, paired, stride=1, steps=None):
    size = len(items)
    steps = steps or range(size)
    if paired:
        return [items[0]] + [
            lax.ppermute(
                items[index],
                axis,
                [(one, one ^ steps[index] * stride) for one in range(size * stride)],
            )
            for index in range(1, size)
        ]
    members = [list(range(first, size * stride, stride)) for first in range(stride)]
    received = lax.all_to_all(
        jnp.stack(items), axis, 0, 0, tiled=True, axis_index_groups=members
    )
    return [received[index] for index in range(size)]


def tree_sum(parts):
    while len(parts) > 1:
        parts = [left + right for left, right in zip(parts[::2], parts[1::2], strict=True)]
    return parts[0]


def norm_kernel(stream_hbm, gain_hbm, *refs, paired, steps):
    normed_ref, *out_refs, stream_ref, gain_ref, sems = refs
    copies = [
        pltpu.make_async_copy(stream_hbm, stream_ref, sems.at[0]),
        pltpu.make_async_copy(gain_hbm, gain_ref, sems.at[1]),
    ]
    for copy in copies:
        copy.start()
    for copy in copies:
        copy.wait()
    width = out_refs[0].shape[1]
    normed_ref[...] = normalized(stream_ref[...].astype(F32), gain_ref[...]).astype(BF16)
    for index, out_ref in enumerate(out_refs):
        group = lax.axis_index("ep") ^ steps[index] if paired else index
        out_ref[...] = normed_ref[:, pl.ds(pl.multiple_of(group * width, width), width)]


def project_kernel(*refs):
    groups = (len(refs) - 3) // 2
    block_refs, weight_refs, out_refs = refs[:groups], refs[groups:-groups], refs[-groups:]
    count = block_refs[0].shape[0]
    width = weight_refs[0].shape[1]
    rows = jnp.concatenate([block_ref[...] for block_ref in block_refs], axis=0)
    query, key, value = [
        jnp.dot(rows, weight_ref[...], preferred_element_type=F32) for weight_ref in weight_refs
    ]
    high = query.astype(BF16)
    low = (query - high.astype(F32)).astype(BF16)
    terms = (high, low, key.astype(BF16), value.astype(BF16))
    for group, out_ref in enumerate(out_refs):
        for index, term in enumerate(terms):
            out_ref[:, index * width : (index + 1) * width] = term[
                group * count : (group + 1) * count
            ]


def attend_kernel(
    lengths_ref,
    normed_ref,
    forget_ref,
    bias_ref,
    gates_ref,
    output_ref,
    keys_ref,
    values_ref,
    *refs,
):
    *part_refs, keep_ref, give_ref, attended_ref, product_ref, scores_ref = refs
    count = normed_ref.shape[0]
    heads = gates_ref.shape[1]
    cache_len = gates_ref.shape[2]
    width = keys_ref.shape[2]
    head_dim = width // heads
    scale = head_dim ** (-0.5)

    forget_all = jax.nn.log_sigmoid(
        dot_transposed(normed_ref[...], forget_ref[...]) + bias_ref[...]
    )
    head_ids = lax.broadcasted_iota(jnp.int32, forget_all.shape, 1)
    first_head = lax.axis_index("tp") * heads
    total = part_refs[0][...].astype(F32)
    for part_ref in part_refs[1:]:
        total = total + part_ref[...].astype(F32)
    query = (total[:, :width] + total[:, width : 2 * width]).astype(BF16).astype(F32)
    key_new = total[:, 2 * width : 3 * width].astype(BF16).astype(F32)
    value_new = total[:, 3 * width :].astype(BF16).astype(F32)
    lanes = lax.broadcasted_iota(jnp.int32, (ROWS, width), 1)
    row_ids = lax.broadcasted_iota(jnp.int32, (ROWS, 1), 0)
    positions = lax.broadcasted_iota(jnp.int32, (ROWS, cache_len), 1)

    def stacked(first):
        return jnp.concatenate(
            [
                jnp.where(lanes // head_dim == head, query[first : first + ROWS], 0.0).astype(BF16)
                for head in range(heads)
            ],
            axis=0,
        )

    for pair in range(0, count, 2 * ROWS):
        streamed, loaded = stacked(pair), stacked(pair + ROWS)
        lane_row = lax.broadcasted_iota(jnp.int32, (BLOCK, heads * ROWS), 1) % ROWS
        loaded_row = lax.broadcasted_iota(jnp.int32, (heads * ROWS, BLOCK), 0) % ROWS
        for start in range(0, cache_len, BLOCK):
            block = slice(start, start + BLOCK)
            down = jnp.zeros((BLOCK, heads * ROWS), F32)
            over = jnp.zeros((heads * ROWS, BLOCK), F32)
            for row in range(ROWS):
                products = dot_transposed(keys_ref[pair + row, block, :], streamed)
                down = jnp.where(lane_row == row, products, down)
                products = dot_transposed(loaded, keys_ref[pair + ROWS + row, block, :])
                over = jnp.where(loaded_row == row, products, over)
            base = heads * pair
            scores_ref[base : base + heads * ROWS, block] = down.T
            scores_ref[base + heads * ROWS : base + 2 * heads * ROWS, block] = over

    for first in range(0, count, ROWS):
        mine = slice(first, first + ROWS)
        length = jnp.zeros((ROWS, 1), jnp.int32)
        for row in range(ROWS):
            length = jnp.where(row_ids == row, lengths_ref[first + row], length)
        base = heads * first
        scores = [
            scores_ref[base + head * ROWS : base + (head + 1) * ROWS, :] for head in range(heads)
        ]
        weights = []
        owns = []
        for head in range(heads):
            gates = gates_ref[mine, head, :]
            columns = slice(head * head_dim, (head + 1) * head_dim)
            last_gate = jnp.sum(
                jnp.where(positions == length - 1, gates, 0.0), axis=1, keepdims=True
            )
            forget_new = jnp.sum(
                jnp.where(head_ids[mine] == first_head + head, forget_all[mine], 0.0),
                axis=1,
                keepdims=True,
            )
            own_score = (
                jnp.sum(query[mine, columns] * key_new[mine, columns], axis=1, keepdims=True)
                * scale
            )
            score = scores[head] * scale + forget_new + last_gate - gates
            score = jnp.where(positions < length, score, HIDDEN)
            largest = jnp.maximum(jnp.max(score, axis=1, keepdims=True), own_score)
            past = jnp.exp(score - largest)
            own_term = jnp.exp(own_score - largest)
            norm = jnp.sum(past, axis=1, keepdims=True) + own_term
            weights.append((past / norm).astype(BF16))
            owns.append((own_term / norm).astype(BF16).astype(F32))
        weights = jnp.concatenate(weights, axis=0)
        results = [
            owns[head] * value_new[mine, head * head_dim : (head + 1) * head_dim]
            for head in range(heads)
        ]
        for row in range(ROWS):
            products = jnp.dot(weights, values_ref[first + row], preferred_element_type=F32)
            for head in range(heads):
                columns = slice(head * head_dim, (head + 1) * head_dim)
                results[head] = results[head] + jnp.where(
                    row_ids == row, products[head * ROWS : (head + 1) * ROWS, columns], 0.0
                )
        for head in range(heads):
            attended_ref[mine, head * head_dim : (head + 1) * head_dim] = results[head]

    attended = attended_ref[...].astype(BF16)
    half = keep_ref.shape[1]
    core = lax.axis_index("tp") % 2
    product_ref[...] = jnp.dot(attended, output_ref[...], preferred_element_type=F32)
    keep_ref[...] = product_ref[:, pl.ds(pl.multiple_of(core * half, half), half)]
    give_ref[...] = product_ref[:, pl.ds(pl.multiple_of((1 - core) * half, half), half)].astype(
        BF16
    )


def pair_kernel(keep_ref, taken_ref, out_ref):
    out_ref[...] = (keep_ref[...].astype(F32) + taken_ref[...].astype(F32)).astype(BF16)


def mix_kernel(stream_ref, *refs):
    *part_refs, out_ref = refs
    half = out_ref.shape[1]
    total = tree_sum([part_ref[...].astype(F32) for part_ref in part_refs])
    mine = pl.ds(pl.multiple_of(lax.axis_index("tp") % 2 * half, half), half)
    out_ref[...] = (stream_ref[:, mine].astype(F32) + total).astype(BF16)


def second_norm_kernel(near_ref, far_ref, gain_ref, normed_ref, mixed_ref, row_ref):
    half = near_ref.shape[1]
    piece = mixed_ref.shape[1]
    place = lax.axis_index("tp")
    row_ref[:, pl.ds(pl.multiple_of(place % 2 * half, half), half)] = near_ref[...].astype(F32)
    row_ref[:, pl.ds(pl.multiple_of((1 - place % 2) * half, half), half)] = far_ref[...].astype(
        F32
    )
    normed_ref[...] = normalized(row_ref[...], gain_ref[...]).astype(BF16)
    mixed_ref[...] = row_ref[:, pl.ds(pl.multiple_of(place * piece, piece), piece)].astype(BF16)


def expert_kernel(
    routes_ref, weights_ref, gate_ref, up_ref, down_ref, *refs, groups, paired
):
    row_refs, (keep_ref, give_ref) = refs[:groups], refs[groups:]
    count = row_refs[0].shape[0]
    piece = keep_ref.shape[2]
    pieces = keep_ref.shape[0] // groups
    half = count // 2
    expert = lax.axis_index("ep")
    rows = jnp.concatenate([row_ref[...] for row_ref in row_refs], axis=0)
    hidden = []
    for start in range(0, gate_ref.shape[1], BLOCK):
        units = slice(start, min(start + BLOCK, gate_ref.shape[1]))
        gated, upper = 0.0, 0.0
        for first in range(0, rows.shape[1], BLOCK):
            features = slice(first, first + BLOCK)
            gated += dot_transposed(rows[:, features], gate_ref[0, units, features])
            upper += dot_transposed(up_ref[0, units, features], rows[:, features])
        hidden.append((gated / (1.0 + jnp.exp(-gated)) * upper.T).astype(BF16))
    hidden = jnp.concatenate(hidden, axis=1)
    partial = jnp.dot(hidden, down_ref[0], preferred_element_type=F32)
    share = jnp.sum(jnp.where(routes_ref[...] == expert, weights_ref[...], 0.0), axis=0, keepdims=True)
    square = (groups * count, groups * count)
    row = lax.broadcasted_iota(jnp.int32, square, 0)
    group = row // count ^ expert if paired else row // count
    same = group * count + row % count == lax.broadcasted_iota(jnp.int32, square, 1)
    share = jnp.sum(jnp.where(same, share, 0.0), axis=1, keepdims=True)
    partial = partial * share
    first_core = lax.axis_index("tp") % 2 == 0
    for index in range(groups):
        lower = partial[index * count : index * count + half]
        upper = partial[index * count + half : (index + 1) * count]
        keep = jnp.where(first_core, lower, upper).astype(BF16)
        give = jnp.where(first_core, upper, lower).astype(BF16)
        group = expert ^ index if paired else index
        for step in range(pieces):
            columns = slice(step * piece, (step + 1) * piece)
            keep_ref[group * pieces + step] = keep[:, columns]
            give_ref[group * pieces + step] = give[:, columns]


def finish_kernel(parts_ref, mixed_ref, out_ref):
    half = parts_ref.shape[1]
    for core in range(2):
        mine = slice(core * half, (core + 1) * half)
        total = mixed_ref[...].astype(F32)[mine]
        for index in range(core, parts_ref.shape[0], 2):
            total = total + parts_ref[index].astype(F32)
        out_ref[mine, :] = total.astype(BF16)


def shards(
    stream,
    norm_gain_attn,
    w_query,
    w_key,
    w_value,
    w_forget,
    forget_bias,
    key_cache,
    value_cache,
    gate_cache,
    lengths,
    w_output,
    norm_gain_ffn,
    routes,
    route_weights,
    w_expert_gate,
    w_expert_up,
    expert_down_weight,
):
    count, model_width = stream.shape
    groups = lax.axis_size("ep")
    pieces = lax.axis_size("tp")
    piece = model_width // pieces
    width = key_cache.shape[2]
    shape = jax.ShapeDtypeStruct
    in_vmem = pl.BlockSpec(memory_space=pltpu.VMEM)
    in_smem = pl.BlockSpec(memory_space=pltpu.SMEM)

    paired = groups in (2, 4)
    steps = (0, 3, 1, 2) if groups == 4 else tuple(range(groups))
    normed, *blocks = call(
        functools.partial(norm_kernel, paired=paired, steps=steps),
        "norm",
        2 * MIB,
        [shape(stream.shape, BF16)] + [shape((count, model_width // groups), BF16)] * groups,
        flops=COVER,
        in_specs=[pl.BlockSpec(memory_space=pltpu.HBM)] * 2,
        scratch_shapes=[
            pltpu.VMEM(stream.shape, BF16),
            pltpu.VMEM((1, model_width), F32),
            pltpu.SemaphoreType.DMA((2,)),
        ],
    )(
        pltpu.with_memory_space_constraint(stream, pltpu.HBM),
        pltpu.with_memory_space_constraint(norm_gain_attn.reshape(1, -1), pltpu.HBM),
    )
    blocks = exchange(blocks, "ep", paired, steps=steps)
    parts = call(
        project_kernel, "project", 4 * MIB, [shape((count, 4 * width), BF16)] * groups
    )(*blocks, w_query, w_key, w_value)
    parts = exchange(parts, "ep", paired, steps=steps)
    swap = [(one, one ^ 1) for one in range(pieces)]
    side = shape((count, model_width // 2), BF16)
    keep, give = call(
        attend_kernel,
        "attend",
        4 * MIB,
        [shape(side.shape, F32), side],
        in_specs=[in_smem] + [in_vmem] * (7 + groups),
        scratch_shapes=[
            pltpu.VMEM((count, width), F32),
            pltpu.VMEM((count, model_width), F32),
            pltpu.VMEM((gate_cache.shape[1] * count, gate_cache.shape[2]), F32),
        ],
    )(
        lengths,
        normed,
        w_forget.T,
        forget_bias.reshape(1, -1),
        gate_cache,
        w_output,
        key_cache,
        value_cache,
        *parts,
    )
    taken = lax.ppermute(give, "tp", swap)
    pair = call(pair_kernel, "pair", MIB, side)(keep, taken)
    chips = pieces // 2
    pair_parts = exchange([pair] * chips, "tp", chips in (2, 4), 2)
    near = call(mix_kernel, "mix", 2 * MIB, side)(stream, *pair_parts)
    far = lax.ppermute(near, "tp", swap)
    rows, mixed = call(
        second_norm_kernel,
        "second_norm",
        2 * MIB,
        [shape(stream.shape, BF16), shape((count, piece), BF16)],
        scratch_shapes=[pltpu.VMEM(stream.shape, F32)],
    )(near, far, norm_gain_ffn.reshape(1, -1))
    half = count // 2
    slots = groups * pieces
    keep, give = call(
        functools.partial(expert_kernel, groups=groups, paired=paired),
        "experts",
        8 * MIB,
        [shape((slots, half, piece), BF16)] * 2,
    )(
        routes.T,
        route_weights.T,
        jnp.swapaxes(w_expert_gate, 1, 2),
        jnp.swapaxes(w_expert_up, 1, 2),
        expert_down_weight,
        *exchange([rows] * groups, "ep", paired),
    )
    taken = lax.ppermute(give, "tp", swap)
    summed = call(pair_kernel, "sides", 4 * MIB, shape((slots, half, piece), BF16))(keep, taken)
    returned = lax.all_to_all(summed, ("ep", "tp"), 0, 0, tiled=True)
    return call(finish_kernel, "finish", 4 * MIB, shape((count, piece), BF16))(returned, mixed)


def solution(mesh):
    placed = (
        P("ep", None),
        P(),
        P("ep", "tp"),
        P("ep", "tp"),
        P("ep", "tp"),
        P(),
        P(),
        P("ep", None, "tp"),
        P("ep", None, "tp"),
        P("ep", "tp", None),
        P("ep"),
        P("tp", None),
        P(),
        P(),
        P(),
        P("ep", None, "tp"),
        P("ep", None, "tp"),
        P("ep", "tp", None),
    )
    return jax.shard_map(
        shards, mesh=mesh, in_specs=placed, out_specs=P("ep", "tp"), check_vma=False
    )
```
